512 devices in a mesh: sp: 256 (over z, y, x), tp: 2 (over core).
Axes of the slice: x: 4, y: 8, z: 8, core: 2. Of those that a mesh axis runs over, the one named last changes fastest.
Arguments:
- tokens: bfloat16 [131072, 2048], P(('sp', 'tp')), may hold values from -6 to 6
- norm_gain: float32 [2048], replicated, may hold values from 0.1 to 1.9
- in_weight: bfloat16 [2048, 1024], P(None, 'tp'), may hold values from -0.125 to 0.125
- gate_weight: bfloat16 [2048, 1024], P(None, 'tp'), may hold values from -0.125 to 0.125
- conv_weight: float32 [4, 1024], P(None, 'tp'), may hold values from -3 to 3
- decay_gate_weight: bfloat16 [16, 64, 64], P('tp'), may hold values from -0.75 to 0.75
- decay_gate_bias: float32 [1024], P('tp'), may hold values from -4 to 4
- input_gate_weight: bfloat16 [16, 64, 64], P('tp'), may hold values from -0.75 to 0.75
- input_gate_bias: float32 [1024], P('tp'), may hold values from -4 to 4
- channel_decay_rate: float32 [1024], P('tp'), may hold values from 3.0517578e-07 to 0.01
- forgetting_offset: float32 [16, 131072], P('tp', 'sp'), may hold values from -1.6 to 0
- out_weight: bfloat16 [1024, 2048], P('tp'), may hold values from -0.1875 to 0.1875
Outputs:
- mixed: bfloat16 [131072, 2048], P(('sp', 'tp'))
The draws below stay inside these ranges and needn't reach their ends.
All inputs are finite; a program needn't handle non-finite values.
Results may differ from the reference program's by a relative error of at most 0.0067.
Values may be sent and summed in bfloat16 or wider, within the bound.
No kernel may reach another device: no remote copies, remote signals or barrier semaphores. Data moves between devices by JAX's collectives and lax.ppermute only.
A program may use at most 64 MiB of HBM per device.

```python
import math
import jax
import jax.numpy as jnp
from jax import lax

D = 2048
HEADS = 16
BLOCK = 64
CONV = 4
TOK_DEV = 256
WIDTH = 1024
GROUP = 512
TOKENS = 131072
N_SP = 256
N_TP = 2


def draw_channel_decay_rate(key, part):
    width = HEADS * BLOCK
    key_pick = jax.random.fold_in(key, 11)
    key_fast = jax.random.fold_in(key, 12)
    key_slow = jax.random.fold_in(key, 13)
    share = 50
    picked = jax.random.randint(key_pick, (width,), 0, 100) < share
    fast_rate = jnp.exp(jax.random.uniform(key_fast, (width,), jnp.float32, math.log(0.003), math.log(0.01)))
    slow_rate = jnp.exp(jax.random.uniform(key_slow, (width,), jnp.float32, math.log(0.04), math.log(0.08))) / TOKENS
    return jnp.where(picked, fast_rate, slow_rate).astype(jnp.float32)


def draw_forgetting_offset(key, part):
    count = TOKENS // GROUP
    key_factor = jax.random.fold_in(key, 21)
    key_spot = jax.random.fold_in(key, 22)
    key_loss = jax.random.fold_in(key, 23)
    factor = jnp.exp(jax.random.uniform(key_factor, (HEADS, count), jnp.float32, 0.0, math.log(4.0)))
    steady_threshold = -(0.2 / TOKENS) * jnp.repeat(factor, GROUP, axis=1)
    spots = jax.random.randint(key_spot, (HEADS, 3, 1), 0, TOKENS)
    objective_terms = jax.random.uniform(key_loss, (HEADS, 3, 1), jnp.float32, 0.22, 0.5)
    assigned_locations = jnp.arange(TOKENS, dtype=jnp.int32)[None, None, :] == spots
    contiguous_intervals = jnp.sum(jnp.where(assigned_locations, -objective_terms, 0.0), axis=1)
    return (steady_threshold + contiguous_intervals).astype(jnp.float32)


def levels(own_key, extent, cuts, smallest, largest):
    factor_of, own = 1.0, jax.random.fold_in(own_key, 6)
    for position, parts in cuts:
        steps = jnp.exp(jax.random.uniform(jax.random.fold_in(own, position), (parts,), jnp.float32, smallest / len(cuts), largest / len(cuts)))
        factor_of = factor_of * jnp.repeat(steps, extent[position] // parts).reshape([-1 if axis == position else 1 for axis in range(len(extent))])
    return factor_of


def noise(key, shape, deviation, bound, shards=(), held_as=jnp.bfloat16):
    loudness = levels(key, shape, shards, -0.22, 0.18) if shards else 1.0
    drawn = jax.random.normal(key, shape, jnp.float32) * deviation * loudness
    return jnp.minimum(jnp.maximum(drawn, -bound), bound).astype(held_as)


def setup_inputs(seed: int = 0) -> dict:
    key_list = jax.random.split(jax.random.key(seed), 13)
    tokens = noise(key_list[0], (TOKENS, D), 1.0, 6.0, ((0, 512),))
    norm_gain = jnp.clip(1.0 + 0.18 * jax.random.normal(key_list[1], (D,), jnp.float32), 0.1, 1.9)
    in_weight = noise(key_list[2], (D, WIDTH), D ** -0.5, 0.125, ((1, 2),))
    gate_weight = noise(key_list[3], (D, WIDTH), D ** -0.5, 0.125, ((1, 2),))
    conv_weight = noise(key_list[4], (CONV, WIDTH), CONV ** -0.5, 3.0, ((1, 2),), jnp.float32)
    decay_gate_weight = noise(key_list[5], (HEADS, BLOCK, BLOCK), BLOCK ** -0.5, 0.75, ((0, 2),))
    decay_gate_bias = noise(key_list[6], (WIDTH,), 1.0, 4.0, ((0, 2),), jnp.float32)
    input_gate_weight = noise(key_list[7], (HEADS, BLOCK, BLOCK), BLOCK ** -0.5, 0.75, ((0, 2),))
    input_gate_bias = noise(key_list[8], (WIDTH,), 1.0, 4.0, ((0, 2),), jnp.float32)
    channel_decay_rate = draw_channel_decay_rate(jax.random.fold_in(key_list[12], 71), 0)
    forgetting_offset = draw_forgetting_offset(jax.random.fold_in(key_list[12], 71), 0)
    out_weight = noise(key_list[11], (WIDTH, D), WIDTH ** -0.5, 0.1875, ((0, 2),))
    return {"tokens": tokens, "norm_gain": norm_gain, "in_weight": in_weight, "gate_weight": gate_weight, "conv_weight": conv_weight, "decay_gate_weight": decay_gate_weight, "decay_gate_bias": decay_gate_bias, "input_gate_weight": input_gate_weight, "input_gate_bias": input_gate_bias, "channel_decay_rate": channel_decay_rate, "forgetting_offset": forgetting_offset, "out_weight": out_weight}


epsilon = 1e-05

def link(earlier, later):
    return (earlier[0] * later[0], later[0] * earlier[1] + later[1])

def reference(tokens, norm_gain, in_weight, gate_weight, conv_weight, decay_gate_weight, decay_gate_bias, input_gate_weight, input_gate_bias, channel_decay_rate, forgetting_offset, out_weight):
    length = TOK_DEV * N_TP
    count = N_SP
    width = HEADS * BLOCK
    token_blocks = tokens.reshape(count, length, D)
    shift_blocks = forgetting_offset.reshape(HEADS, count, length).transpose(1, 2, 0)

    def advance(carry, item):
        prior, tail = carry
        interval_matrix_lines, shift_rows = item
        floats = interval_matrix_lines.astype(jnp.float32)
        middle_point = floats - lax.optimization_barrier(jnp.mean(floats, axis=1, keepdims=True))
        spread = lax.optimization_barrier(jnp.mean(middle_point * middle_point, axis=1, keepdims=True))
        normed = (middle_point * lax.rsqrt(spread + epsilon) * norm_gain).astype(jnp.bfloat16)
        inner = jnp.dot(normed, in_weight, preferred_element_type=jnp.float32).astype(jnp.bfloat16)
        gate = jnp.dot(normed, gate_weight, preferred_element_type=jnp.float32).astype(jnp.bfloat16)
        extended = jnp.concatenate([tail, inner], axis=0)
        smooth = extended[0:length].astype(jnp.float32) * conv_weight[0]
        for tap in range(1, CONV):
            smooth = smooth + extended[tap:tap + length].astype(jnp.float32) * conv_weight[tap]
        smoothed = smooth.astype(jnp.bfloat16)
        grouped = smoothed.astype(jnp.float32).reshape(length, HEADS, BLOCK)
        retain = jax.nn.sigmoid(jnp.einsum('rhi,hij->rhj', grouped, decay_gate_weight.astype(jnp.float32)).reshape(length, width) + decay_gate_bias)
        admit = jax.nn.sigmoid(jnp.einsum('rhi,hij->rhj', grouped, input_gate_weight.astype(jnp.float32)).reshape(length, width) + input_gate_bias)
        log_decay = -8.0 * retain * channel_decay_rate + jnp.repeat(shift_rows, BLOCK, axis=1)
        decay = jnp.exp(log_decay)
        drive = jnp.sqrt(-jnp.expm1(2.0 * log_decay)) * admit * smoothed.astype(jnp.float32)
        product, local = lax.associative_scan(link, (decay, drive), axis=0)
        state = local + product * prior
        gated = (state * jax.nn.gelu(gate.astype(jnp.float32))).astype(jnp.bfloat16)
        result = jnp.dot(gated, out_weight, preferred_element_type=jnp.float32).astype(jnp.bfloat16)
        return ((state[length - 1], inner[length - CONV + 1:]), result)
    start = (jnp.zeros((width,), jnp.float32), jnp.zeros((CONV - 1, width), jnp.bfloat16))
    _, results = lax.scan(advance, start, (token_blocks, shift_blocks))
    return results.reshape(TOKENS, D)
```

```python
import functools

import jax
import jax.numpy as jnp
from jax import lax
from jax.experimental import pallas as pl
from jax.experimental.pallas import tpu as pltpu
from jax.sharding import Mesh
from jax.sharding import PartitionSpec as P

SP = ("sp_0", "sp_1", "sp_2")
PLANE = ("sp_1", "sp_2")
SP_TP = ("sp_0", "sp_1", "sp_2", "tp")

EPSILON = 1e-05
SUB = 8
HALO = 8
f32, bf16 = jnp.float32, jnp.bfloat16


def dot(a, b):
    return jnp.dot(a, b, preferred_element_type=f32)


def normalized(x, gain):
    x = x.astype(f32)
    centered = x - jnp.mean(x, axis=1, keepdims=True)
    spread = jnp.mean(centered * centered, axis=1, keepdims=True)
    return centered * lax.rsqrt(spread + EPSILON) * gain


def sigmoid(x):
    return 1.0 / (1.0 + jnp.exp(-x))


def one_minus_exp(z, e):
    series = 1.0 - z * (1.0 / 7.0)
    for k in (6, 5, 4, 3, 2):
        series = 1.0 - z * (1.0 / k) * series
    return jnp.where(z < 0.3, z * series, 1.0 - e)


def local_kernel(
    own, other, halo_a, halo_b, gain, w_in, w_gate, conv, w_decay, b_decay, w_input, b_input, rate, offset,
    h_out, p_out, g_out, runs_out, sent_out,
    normed, before, smoothed, pre_r, pre_i, shift, blocks, extended,
):
    half, width = own.shape[0], w_in.shape[1]
    length = 2 * half
    run = length // SUB
    taps = conv.shape[0]
    lead = (taps - 1) * SUB
    tp = lax.axis_index("tp")

    halo = normalized(jnp.where(tp == 1, halo_a[...].astype(f32), halo_b[...].astype(f32)), gain[...])
    before[...] = jnp.concatenate([halo, jnp.zeros_like(halo)], axis=0).astype(bf16)
    step = 16
    for source, base in ((own, tp * half), (other, (1 - tp) * half)):

        def norm_rows(i, _, source=source, base=base):
            r = pl.multiple_of(i * step, step)
            d = pl.multiple_of(base + i * step, step)
            normed[pl.ds(d, step), :] = normalized(source[pl.ds(r, step), :], gain[...]).astype(bf16)
            return 0

        lax.fori_loop(0, half // step, norm_rows, 0, unroll=2)

    inner = dot(normed[...], w_in[...]).astype(bf16)
    inner_before = dot(before[...], w_in[...]).astype(bf16)
    gate = dot(normed[...], w_gate[...]).astype(bf16)

    def picks(rows, first, cols, base):
        r = lax.broadcasted_iota(jnp.int32, (rows, cols), 0)
        c = lax.broadcasted_iota(jnp.int32, (rows, cols), 1)
        return jnp.where(c == (r & (SUB - 1)) * run + (r >> 3) + first + base, 1.0, 0.0).astype(bf16)

    order = picks(length, 0, length, 0)
    extended[pl.ds(lead, length), :] = dot(order, inner)
    r = lax.broadcasted_iota(jnp.int32, (lead, 2 * HALO), 0)
    c = lax.broadcasted_iota(jnp.int32, (lead, 2 * HALO), 1)
    from_halo = jnp.where(((r & (SUB - 1)) == 0) & (c == (r >> 3) + HALO - taps + 1), 1.0, 0.0).astype(bf16)
    extended[pl.ds(0, lead), :] = dot(picks(lead, 1 - taps, length, 0), inner) + dot(from_halo, inner_before)
    g_out[...] = jax.nn.gelu(dot(order, gate))

    smooth = extended[pl.ds(0, length), :] * conv[0:1, :]
    for tap in range(1, taps):
        smooth = smooth + extended[pl.ds(tap * SUB, length), :] * conv[tap : tap + 1, :]
    smoothed[...] = smooth.astype(bf16)

    heads, block = w_decay.shape[0], w_decay.shape[1]
    wide = 256
    per = wide // block
    blocks[...] = jnp.zeros_like(blocks)
    for head in range(heads):
        q, i = head // per, (head % per) * block
        blocks[q, pl.ds(i, block), pl.ds(i, block)] = w_decay[head]
        blocks[q, pl.ds(i, block), pl.ds(wide + i, block)] = w_input[head]
    for q in range(heads // per):
        both = dot(smoothed[:, q * wide : (q + 1) * wide], blocks[q])
        pre_r[:, q * wide : (q + 1) * wide] = both[:, :wide]
        pre_i[:, q * wide : (q + 1) * wide] = both[:, wide:]

    part0 = offset[...].astype(bf16).astype(f32)
    part1 = (offset[...] - part0).astype(bf16).astype(f32)
    part2 = offset[...] - part0 - part1
    parts = jnp.concatenate([part0, part1, part2, jnp.zeros_like(part0)], axis=0).astype(bf16)
    moved = lax.dot_general(parts, order, (((1,), (1,)), ((), ())), preferred_element_type=f32).astype(bf16)
    r = lax.broadcasted_iota(jnp.int32, (4 * heads, width), 0)
    c = lax.broadcasted_iota(jnp.int32, (4 * heads, width), 1)
    spread = jnp.where((r & (heads - 1)) == (c >> 6), 1.0, 0.0).astype(bf16)
    shift[...] = lax.dot_general(moved, spread, (((0,), (0,)), ((), ())), preferred_element_type=f32)

    rows = 4 * SUB

    def scan_rows(i, carry):
        h, p = carry
        at = pl.ds(pl.multiple_of(i * rows, rows), rows)
        x = smoothed[at, :].astype(f32)
        retain = sigmoid(pre_r[at, :] + b_decay[...])
        admit = sigmoid(pre_i[at, :] + b_input[...])
        log_decay = -8.0 * retain * rate[...] + shift[at, :]
        decay = jnp.exp(log_decay)
        drive = jnp.sqrt(one_minus_exp(-2.0 * log_decay, decay * decay)) * admit * x
        for k in range(rows // SUB):
            a = decay[k * SUB : (k + 1) * SUB, :]
            h = a * h + drive[k * SUB : (k + 1) * SUB, :]
            p = a * p
            here = pl.ds(pl.multiple_of(i * rows + k * SUB, SUB), SUB)
            h_out[here, :] = h
            p_out[here, :] = p
        return h, p

    h, p = lax.fori_loop(
        0, length // rows, scan_rows, (jnp.zeros((SUB, width), f32), jnp.ones((SUB, width), f32))
    )
    a_before, b_before = jnp.ones((1, width), f32), jnp.zeros((1, width), f32)
    for s in range(SUB):
        runs_out[0, s : s + 1, :] = a_before
        runs_out[1, s : s + 1, :] = b_before
        a_before, b_before = a_before * p[s : s + 1, :], p[s : s + 1, :] * b_before + h[s : s + 1, :]
    pair = jnp.concatenate([a_before, b_before], axis=0)
    sent_out[...] = jnp.broadcast_to(pair[None], sent_out.shape)


def before_in(pieces, index):
    width = pieces.shape[2]
    a, b = jnp.ones((1, width), f32), jnp.zeros((1, width), f32)
    a_at, b_at = a, b
    for k in range(pieces.shape[0]):
        here = k == index
        a_at, b_at = jnp.where(here, a, a_at), jnp.where(here, b, b_at)
        a_k, b_k = pieces[k, 0:1, :], pieces[k, 1:2, :]
        a, b = a * a_k, a_k * b + b_k
    return (a_at, b_at), (a, b)


def plane_kernel(pieces, before_out, sent_out):
    index = lax.axis_index("sp_1") * lax.axis_size("sp_2") + lax.axis_index("sp_2")
    (a_at, b_at), (a, b) = before_in(pieces, index)
    before_out[...] = jnp.concatenate([a_at, b_at], axis=0)
    pair = jnp.concatenate([a, b], axis=0)
    sent_out[...] = jnp.broadcast_to(pair[None], sent_out.shape)


def state_kernel(pieces, before, runs, h, p, g, mine_out, theirs_out, gated):
    (_, b_at), _ = before_in(pieces, lax.axis_index("sp_0"))
    carried = before[0:1, :] * b_at + before[1:2, :]
    start = runs[0] * carried + runs[1]
    length = h.shape[0]
    half, run = length // 2, length // SUB
    rows = 4 * SUB
    starts = jnp.concatenate([start] * (rows // SUB), axis=0)

    def state_rows(i, _):
        at = pl.ds(pl.multiple_of(i * rows, rows), rows)
        gated[at, :] = ((h[at, :] + p[at, :] * starts) * g[at, :]).astype(bf16)
        return 0

    lax.fori_loop(0, length // rows, state_rows, 0, unroll=2)
    tp = lax.axis_index("tp")

    def back(first):
        t = lax.broadcasted_iota(jnp.int32, (half, length), 0) + first
        c = lax.broadcasted_iota(jnp.int32, (half, length), 1)
        pick = jnp.where(t == (c & (SUB - 1)) * run + (c >> 3), 1.0, 0.0).astype(bf16)
        return dot(pick, gated[...]).astype(bf16)

    theirs_out[...] = back((1 - tp) * half)
    mine_out[...] = back(tp * half)


def out_kernel(mine, theirs, w_mine, w_theirs, out):
    out[...] = (dot(mine[...], w_mine[...]) + dot(theirs[...], w_theirs[...])).astype(bf16)


def call(kernel, name, out_shape, scratch=(), **kw):
    return pl.pallas_call(
        kernel,
        out_shape=out_shape,
        scratch_shapes=list(scratch),
        compiler_params=pltpu.CompilerParams(vmem_limit_bytes=60000 * 1024),
        name=name,
        **kw,
    )


def body(
    tokens,
    norm_gain,
    in_weight,
    gate_weight,
    conv_weight,
    decay_gate_weight,
    decay_gate_bias,
    input_gate_weight,
    input_gate_bias,
    channel_decay_rate,
    forgetting_offset,
    out_weight,
):
    half, features = tokens.shape
    length = 2 * half
    width = in_weight.shape[1]
    heads, block = decay_gate_weight.shape[:2]
    count = lax.axis_size(SP)
    plane = lax.axis_size(PLANE)
    deep = lax.axis_size("sp_0")
    S = jax.ShapeDtypeStruct

    swap = [(0, 1), (1, 0)]
    other = lax.ppermute(tokens, "tp", swap)
    tail = tokens[half - HALO :]
    halo_a = lax.ppermute(tail, SP_TP, [(2 * s + 1, 2 * s + 3) for s in range(count - 1)])
    halo_b = lax.ppermute(tail, SP_TP, [(2 * s + 1, 2 * s + 2) for s in range(count - 1)])
    w_theirs = lax.ppermute(out_weight, "tp", swap)

    row = lambda v: v.reshape(1, -1)
    h, p, g, runs, sent = call(
        local_kernel,
        "local_part",
        (
            S((length, width), f32),
            S((length, width), f32),
            S((length, width), f32),
            S((2, SUB, width), f32),
            S((plane, 2, width), f32),
        ),
        scratch=(
            pltpu.VMEM((length, features), bf16),
            pltpu.VMEM((2 * HALO, features), bf16),
            pltpu.VMEM((length, width), bf16),
            pltpu.VMEM((length, width), f32),
            pltpu.VMEM((length, width), f32),
            pltpu.VMEM((length, width), f32),
            pltpu.VMEM((heads * block // 256, 256, 512), bf16),
            pltpu.VMEM((length + (conv_weight.shape[0] - 1) * SUB, width), f32),
        ),
    )(
        tokens, other, halo_a, halo_b, row(norm_gain), in_weight, gate_weight, conv_weight, decay_gate_weight,
        row(decay_gate_bias), input_gate_weight, row(input_gate_bias), row(channel_decay_rate), forgetting_offset,
    )
    pieces = lax.all_to_all(sent, PLANE, split_axis=0, concat_axis=0, tiled=True)
    before, sent = call(
        plane_kernel, "plane_part", (S((2, width), f32), S((deep, 2, width), f32))
    )(pieces)
    pieces = lax.all_to_all(sent, "sp_0", split_axis=0, concat_axis=0, tiled=True)
    mine, theirs = call(
        state_kernel,
        "state_part",
        (S((half, width), bf16), S((half, width), bf16)),
        scratch=(pltpu.VMEM((length, width), bf16),),
    )(pieces, before, runs, h, p, g)
    received = lax.ppermute(theirs, "tp", swap)
    cols = 512
    return call(
        out_kernel,
        "out_part",
        S((half, features), bf16),
        grid=(features // cols,),
        in_specs=[
            pl.BlockSpec((half, width), lambda i: (0, 0)),
            pl.BlockSpec((half, width), lambda i: (0, 0)),
            pl.BlockSpec((width, cols), lambda i: (0, i)),
            pl.BlockSpec((width, cols), lambda i: (0, i)),
        ],
        out_specs=pl.BlockSpec((half, cols), lambda i: (0, i)),
    )(mine, received, out_weight, w_theirs)


def solution(mesh):
    torus = Mesh(mesh.devices.reshape(8, 8, 4, mesh.shape["tp"]), SP_TP)
    placed = (
        P(SP_TP, None),
        P(),
        P(None, "tp"),
        P(None, "tp"),
        P(None, "tp"),
        P("tp", None, None),
        P("tp"),
        P("tp", None, None),
        P("tp"),
        P("tp"),
        P("tp", SP),
        P("tp", None),
    )
    return jax.shard_map(
        body, mesh=torus, in_specs=placed, out_specs=P(SP_TP, None), check_vma=False
    )
```

```python
import jax
import jax.numpy as jnp
from jax import lax
from jax.experimental import pallas as pl
from jax.experimental.pallas import tpu as pltpu
from jax.sharding import Mesh
from jax.sharding import PartitionSpec as P

SP = ("sp_0", "sp_1", "sp_2")
PLANE = ("sp_1", "sp_2")
SP_TP = ("sp_0", "sp_1", "sp_2", "tp")

EPSILON = 1e-05
SUB = 8
HALO = 8
f32, bf16 = jnp.float32, jnp.bfloat16


def dot(a, b):
    return jnp.dot(a, b, preferred_element_type=f32)


def normalized(x, gain):
    x = x.astype(f32)
    centered = x - jnp.mean(x, axis=1, keepdims=True)
    spread = jnp.mean(centered * centered, axis=1, keepdims=True)
    return centered * lax.rsqrt(spread + EPSILON) * gain


def sigmoid(x):
    return 1.0 / (1.0 + jnp.exp(-x))


def local_kernel(
    other, halo_a, halo_b, *refs,
):
    stored, refs = refs[:ARGS], refs[ARGS:]
    h_out, p_out, g_out, runs_out, sent_out, *refs = refs
    held, refs = refs[:ARGS], refs[ARGS:]
    arrived, normed, before, smoothed, pre_r, pre_i, shift, blocks, extended = refs
    copies = [pltpu.make_async_copy(a, b, arrived.at[i]) for i, (a, b) in enumerate(zip(stored, held))]
    for copy in copies:
        copy.start()
    gain, own, w_in, w_gate, conv, w_decay, b_decay, w_input, b_input, rate, offset = held
    half, width = own.shape[0], w_in.shape[1]
    length = 2 * half
    run = length // SUB
    taps = conv.shape[0]
    lead = (taps - 1) * SUB
    tp = lax.axis_index("tp")

    copies[0].wait()
    halo = normalized(jnp.where(tp == 1, halo_a[...].astype(f32), halo_b[...].astype(f32)), gain[...])
    before[...] = jnp.concatenate([halo, jnp.zeros_like(halo)], axis=0).astype(bf16)
    step = 16
    for source, base in ((other, (1 - tp) * half), (own, tp * half)):
        if source is own:
            copies[1].wait()

        def norm_rows(i, _, source=source, base=base):
            r = pl.multiple_of(i * step, step)
            d = pl.multiple_of(base + i * step, step)
            normed[pl.ds(d, step), :] = normalized(source[pl.ds(r, step), :], gain[...]).astype(bf16)
            return 0

        lax.fori_loop(0, half // step, norm_rows, 0, unroll=2)

    copies[2].wait()
    inner = dot(normed[...], w_in[...]).astype(bf16)
    inner_before = dot(before[...], w_in[...]).astype(bf16)
    for copy in copies[3:]:
        copy.wait()
    gate = dot(normed[...], w_gate[...]).astype(bf16)

    def picks(rows, first, cols, base):
        r = lax.broadcasted_iota(jnp.int32, (rows, cols), 0)
        c = lax.broadcasted_iota(jnp.int32, (rows, cols), 1)
        return jnp.where(c == (r & (SUB - 1)) * run + (r >> 3) + first + base, 1.0, 0.0).astype(bf16)

    order = picks(length, 0, length, 0)
    extended[pl.ds(lead, length), :] = dot(order, inner)
    r = lax.broadcasted_iota(jnp.int32, (lead, 2 * HALO), 0)
    c = lax.broadcasted_iota(jnp.int32, (lead, 2 * HALO), 1)
    from_halo = jnp.where(((r & (SUB - 1)) == 0) & (c == (r >> 3) + HALO - taps + 1), 1.0, 0.0).astype(bf16)
    extended[pl.ds(0, lead), :] = dot(picks(lead, 1 - taps, length, 0), inner) + dot(from_halo, inner_before)
    g_out[...] = jax.nn.gelu(dot(order, gate))

    smooth = extended[pl.ds(0, length), :] * conv[0:1, :]
    for tap in range(1, taps):
        smooth = smooth + extended[pl.ds(tap * SUB, length), :] * conv[tap : tap + 1, :]
    smoothed[...] = smooth.astype(bf16)

    heads, block = w_decay.shape[0], w_decay.shape[1]
    wide = 256
    per = wide // block
    blocks[...] = jnp.zeros_like(blocks)
    for head in range(heads):
        q, i = head // per, (head % per) * block
        blocks[q, pl.ds(i, block), pl.ds(i, block)] = w_decay[head]
        blocks[q, pl.ds(i, block), pl.ds(wide + i, block)] = w_input[head]
    for q in range(heads // per):
        both = dot(smoothed[:, q * wide : (q + 1) * wide], blocks[q])
        pre_r[:, q * wide : (q + 1) * wide] = both[:, :wide]
        pre_i[:, q * wide : (q + 1) * wide] = both[:, wide:]

    part0 = offset[...].astype(bf16).astype(f32)
    part1 = (offset[...] - part0).astype(bf16).astype(f32)
    part2 = offset[...] - part0 - part1
    parts = jnp.concatenate([part0, part1, part2, jnp.zeros_like(part0)], axis=0).astype(bf16)
    moved = lax.dot_general(parts, order, (((1,), (1,)), ((), ())), preferred_element_type=f32).astype(bf16)
    r = lax.broadcasted_iota(jnp.int32, (4 * heads, width), 0)
    c = lax.broadcasted_iota(jnp.int32, (4 * heads, width), 1)
    spread = jnp.where((r & (heads - 1)) == (c >> 6), -1.0, 0.0).astype(bf16)
    shift[...] = lax.dot_general(moved, spread, (((0,), (0,)), ((), ())), preferred_element_type=f32)

    rows = 4 * SUB

    def scan_rows(i, carry):
        h, p = carry
        at = pl.ds(pl.multiple_of(i * rows, rows), rows)
        retain = sigmoid(pre_r[at, :] + b_decay[...])
        admit = sigmoid(pre_i[at, :] + b_input[...])
        loss = retain * (8.0 * rate[...]) + shift[at, :]
        decay = jnp.exp(-loss)
        rest = jnp.tanh(loss) * (1.0 + decay * decay)
        drive = rest * lax.rsqrt(jnp.maximum(rest, 1e-37)) * admit * smoothed[at, :].astype(f32)
        for k in range(rows // SUB):
            a = decay[k * SUB : (k + 1) * SUB, :]
            h = a * h + drive[k * SUB : (k + 1) * SUB, :]
            p = a * p
            here = pl.ds(pl.multiple_of(i * rows + k * SUB, SUB), SUB)
            h_out[here, :] = h
            p_out[here, :] = p
        return h, p

    h, p = lax.fori_loop(
        0, length // rows, scan_rows, (jnp.zeros((SUB, width), f32), jnp.ones((SUB, width), f32))
    )
    a_before, b_before = jnp.ones((1, width), f32), jnp.zeros((1, width), f32)
    for s in range(SUB):
        runs_out[0, s : s + 1, :] = a_before
        runs_out[1, s : s + 1, :] = b_before
        a_before, b_before = a_before * p[s : s + 1, :], p[s : s + 1, :] * b_before + h[s : s + 1, :]
    pair = jnp.concatenate([a_before, b_before], axis=0)
    sent_out[...] = jnp.broadcast_to(pair[None], sent_out.shape)


def before_in(pieces, index):
    width = pieces.shape[2]
    a, b = jnp.ones((1, width), f32), jnp.zeros((1, width), f32)
    a_at, b_at = a, b
    for k in range(pieces.shape[0]):
        here = k == index
        a_at, b_at = jnp.where(here, a, a_at), jnp.where(here, b, b_at)
        a_k, b_k = pieces[k, 0:1, :], pieces[k, 1:2, :]
        a, b = a * a_k, a_k * b + b_k
    return (a_at, b_at), (a, b)


def plane_kernel(pieces, before_out, sent_out):
    index = lax.axis_index("sp_1") * lax.axis_size("sp_2") + lax.axis_index("sp_2")
    (a_at, b_at), (a, b) = before_in(pieces, index)
    before_out[...] = jnp.concatenate([a_at, b_at], axis=0)
    pair = jnp.concatenate([a, b], axis=0)
    sent_out[...] = jnp.broadcast_to(pair[None], sent_out.shape)


def state_kernel(pieces, before, runs, h, p, g, mine_out, theirs_out, gated):
    (_, b_at), _ = before_in(pieces, lax.axis_index("sp_0"))
    carried = before[0:1, :] * b_at + before[1:2, :]
    start = runs[0] * carried + runs[1]
    length = h.shape[0]
    half, run = length // 2, length // SUB
    rows = 4 * SUB
    starts = jnp.concatenate([start] * (rows // SUB), axis=0)

    def state_rows(i, _):
        at = pl.ds(pl.multiple_of(i * rows, rows), rows)
        gated[at, :] = ((h[at, :] + p[at, :] * starts) * g[at, :]).astype(bf16)
        return 0

    lax.fori_loop(0, length // rows, state_rows, 0, unroll=2)
    tp = lax.axis_index("tp")

    def back(first):
        t = lax.broadcasted_iota(jnp.int32, (half, length), 0) + first
        c = lax.broadcasted_iota(jnp.int32, (half, length), 1)
        pick = jnp.where(t == (c & (SUB - 1)) * run + (c >> 3), 1.0, 0.0).astype(bf16)
        return dot(pick, gated[...]).astype(bf16)

    theirs_out[...] = back((1 - tp) * half)
    mine_out[...] = back(tp * half)


def out_kernel(mine, theirs, w_mine, w_theirs, out, block, sent):
    cols = block.shape[2]
    copies = []
    for i in range(block.shape[0]):
        at = pl.ds(i * cols, cols)
        block[i] = (dot(mine[...], w_mine[:, at]) + dot(theirs[...], w_theirs[:, at])).astype(bf16)
        copies.append(pltpu.make_async_copy(block.at[i], out.at[:, at], sent.at[i]))
        copies[i].start()
    for copy in copies:
        copy.wait()


VMEM = pl.BlockSpec(memory_space=pltpu.VMEM)


HBM = pl.BlockSpec(memory_space=pltpu.HBM)
ARGS = 11


def call(kernel, name, inputs, out_shape, scratch=(), out_specs=None):
    run = pl.pallas_call(
        kernel,
        out_shape=out_shape,
        out_specs=out_specs or jax.tree.map(lambda _: VMEM, out_shape),
        scratch_shapes=list(scratch),
        compiler_params=pltpu.CompilerParams(vmem_limit_bytes=32 * 1024 * 1024),
        name=name,
        in_specs=[VMEM] * inputs[0] + [HBM] * inputs[1],
    )

    def place(i, a):
        return pltpu.with_memory_space_constraint(a, pltpu.VMEM if i < inputs[0] else pltpu.HBM)

    return lambda *args: run(*(place(i, a) for i, a in enumerate(args)))


def body(
    tokens,
    norm_gain,
    in_weight,
    gate_weight,
    conv_weight,
    decay_gate_weight,
    decay_gate_bias,
    input_gate_weight,
    input_gate_bias,
    channel_decay_rate,
    forgetting_offset,
    out_weight,
):
    half, features = tokens.shape
    length = 2 * half
    width = in_weight.shape[1]
    heads, block = decay_gate_weight.shape[:2]
    count = lax.axis_size(SP)
    plane = lax.axis_size(PLANE)
    deep = lax.axis_size("sp_0")
    S = jax.ShapeDtypeStruct

    swap = [(0, 1), (1, 0)]
    tail = tokens[half - HALO :]
    other = lax.ppermute(tokens, "tp", swap)
    halo_a = lax.ppermute(tail, SP_TP, [(2 * s + 1, 2 * s + 3) for s in range(count - 1)])
    halo_b = lax.ppermute(tail, SP_TP, [(2 * s + 1, 2 * s + 2) for s in range(count - 1)])
    w_theirs = lax.ppermute(out_weight, "tp", swap)

    row = lambda v: v.reshape(1, -1)
    fetched = (
        row(norm_gain), tokens, in_weight, gate_weight, conv_weight, decay_gate_weight, row(decay_gate_bias),
        input_gate_weight, row(input_gate_bias), row(channel_decay_rate), forgetting_offset,
    )
    big = pltpu.VMEM
    h, p, g, runs, sent = call(
        local_kernel,
        "local_part",
        (3, ARGS),
        (
            big((length, width), f32),
            big((length, width), f32),
            big((length, width), f32),
            big((2, SUB, width), f32),
            big((plane, 2, width), f32),
        ),
        scratch=[big(a.shape, a.dtype) for a in fetched]
        + [
            pltpu.SemaphoreType.DMA((ARGS,)),
            big((length, features), bf16),
            big((2 * HALO, features), bf16),
            big((length, width), bf16),
            big((length, width), f32),
            big((length, width), f32),
            big((length, width), f32),
            big((heads * block // 256, 256, 512), bf16),
            big((length + (conv_weight.shape[0] - 1) * SUB, width), f32),
        ],
    )(other, halo_a, halo_b, *fetched)
    pieces = lax.all_to_all(sent, PLANE, split_axis=0, concat_axis=0, tiled=True)
    before, sent = call(
        plane_kernel, "plane_part", (1, 0), (big((2, width), f32), big((deep, 2, width), f32))
    )(pieces)
    pieces = lax.all_to_all(sent, "sp_0", split_axis=0, concat_axis=0, tiled=True)
    mine, theirs = call(
        state_kernel,
        "state_part",
        (6, 0),
        (big((half, width), bf16), big((half, width), bf16)),
        scratch=(big((length, width), bf16),),
    )(pieces, before, runs, h, p, g)
    received = lax.ppermute(theirs, "tp", swap)
    cols = 512
    return call(
        out_kernel,
        "out_part",
        (4, 0),
        S((half, features), bf16),
        scratch=(big((features // cols, half, cols), bf16), pltpu.SemaphoreType.DMA((features // cols,))),
        out_specs=HBM,
    )(mine, received, out_weight, w_theirs)


def solution(mesh):
    torus = Mesh(mesh.devices.reshape(8, 8, 4, mesh.shape["tp"]), SP_TP)
    placed = (
        P(SP_TP, None),
        P(),
        P(None, "tp"),
        P(None, "tp"),
        P(None, "tp"),
        P("tp", None, None),
        P("tp"),
        P("tp", None, None),
        P("tp"),
        P("tp"),
        P("tp", SP),
        P("tp", None),
    )
    return jax.shard_map(
        body, mesh=torus, in_specs=placed, out_specs=P(SP_TP, None), check_vma=False
    )
```

```python
import jax
import jax.numpy as jnp
from jax import lax
from jax.experimental import pallas as pl
from jax.experimental.pallas import tpu as pltpu
from jax.sharding import Mesh
from jax.sharding import PartitionSpec as P

SP = ("sp_0", "sp_1", "sp_2")
PLANE = ("sp_1", "sp_2")
SP_TP = ("sp_0", "sp_1", "sp_2", "tp")

EPSILON = 1e-05
SUB = 8
HALO = 8
f32, bf16 = jnp.float32, jnp.bfloat16


def dot(a, b):
    return jnp.dot(a, b, preferred_element_type=f32)


def normalized(x, gain):
    x = x.astype(f32)
    centered = x - jnp.mean(x, axis=1, keepdims=True)
    spread = jnp.mean(centered * centered, axis=1, keepdims=True)
    return centered * lax.rsqrt(spread + EPSILON) * gain


def sigmoid(x):
    return 1.0 / (1.0 + jnp.exp(-x))


def local_kernel(other, halo_a, halo_b, *refs):
    stored, refs = refs[:ARGS], refs[ARGS:]
    h_out, p_out, g_out, runs_out, sent_out, *refs = refs
    gain, own, conv, w_decay, b_decay, w_input, b_input, rate, offset, *refs = refs
    w_in, w_gate, arrived, normed, middle, scale, smoothed, pre_r, pre_i, shift, blocks, extended = refs
    half, width = own.shape[0], w_in.shape[1]
    held = (gain, w_in, own, w_gate, conv, w_decay, b_decay, w_input, b_input, rate, offset)
    copies = [pltpu.make_async_copy(a, b, arrived.at[i]) for i, (a, b) in enumerate(zip(stored, held))]
    length = 2 * half
    run = length // SUB
    taps = conv.shape[0]
    lead = (taps - 1) * SUB
    tp = lax.axis_index("tp")
    step, lanes = 32, 128
    features = own.shape[1]

    def tiles(source, r):
        return [source[r, t : t + lanes].astype(f32) for t in range(0, features, lanes)]

    def by_rows(one):
        def rows(i, _):
            one(pl.multiple_of(i * step, step))
            return 0

        lax.fori_loop(0, half // step, rows, 0)

    def over_features(stat):
        return jnp.broadcast_to(jnp.sum(stat[...], axis=1, keepdims=True) * (1.0 / features), stat.shape)

    def norm_tokens(source, base, ready=None):
        def add_up(i):
            r = pl.ds(i, step)
            middle[r, :] = sum(tiles(source, r))

        by_rows(add_up)
        middle[...] = over_features(middle)

        def add_squares(i):
            r = pl.ds(i, step)
            m = middle[r, :]
            scale[r, :] = sum((x - m) * (x - m) for x in tiles(source, r))

        by_rows(add_squares)
        scale[...] = lax.rsqrt(over_features(scale) + EPSILON)
        if ready is not None:
            ready.wait()

        def write(i):
            r = pl.ds(i, step)
            m, k = middle[r, :], scale[r, :]
            d = pl.ds(pl.multiple_of(base + i, step), step)
            for t, x in zip(range(0, features, lanes), tiles(source, r)):
                normed[d, t : t + lanes] = ((x - m) * k * gain[:, t : t + lanes]).astype(bf16)

        by_rows(write)

    for i in (0, 2, 1, *range(3, ARGS)):
        copies[i].start()
    norm_tokens(other, (1 - tp) * half, copies[0])
    halo = normalized(jnp.where(tp == 1, halo_a[...].astype(f32), halo_b[...].astype(f32)), gain[...])
    normed[pl.ds(length, 2 * HALO), :] = jnp.concatenate([halo, jnp.zeros_like(halo)], axis=0).astype(bf16)
    copies[2].wait()
    norm_tokens(own, tp * half)
    copies[1].wait()
    both = dot(normed[...], w_in[...]).astype(bf16)
    inner, inner_before = both[:length], both[length:]
    for copy in copies[3:]:
        copy.wait()
    gate = dot(normed[:length, :], w_gate[...]).astype(bf16)

    def picks(rows, base):
        r = lax.broadcasted_iota(jnp.int32, (rows, length), 0)
        c = lax.broadcasted_iota(jnp.int32, (rows, length), 1)
        return jnp.where(c == (r & (SUB - 1)) * run + (r >> 3) + base, 1.0, 0.0).astype(bf16)

    order = picks(length, 0)
    extended[pl.ds(lead, length), :] = dot(order, inner)
    r = lax.broadcasted_iota(jnp.int32, (lead, 2 * HALO), 0)
    c = lax.broadcasted_iota(jnp.int32, (lead, 2 * HALO), 1)
    from_halo = jnp.where(((r & (SUB - 1)) == 0) & (c == (r >> 3) + HALO - taps + 1), 1.0, 0.0).astype(bf16)
    extended[pl.ds(0, lead), :] = dot(picks(lead, 1 - taps), inner) + dot(from_halo, inner_before)
    g_out[...] = jax.nn.gelu(dot(order, gate))

    smooth = extended[pl.ds(0, length), :] * conv[0:1, :]
    for tap in range(1, taps):
        smooth = smooth + extended[pl.ds(tap * SUB, length), :] * conv[tap : tap + 1, :]
    smoothed[...] = smooth.astype(bf16)

    heads, block = w_decay.shape[0], w_decay.shape[1]
    wide = 256
    per = wide // block
    blocks[...] = jnp.zeros_like(blocks)
    for head in range(heads):
        q, i = head // per, (head % per) * block
        blocks[q, pl.ds(i, block), pl.ds(i, block)] = w_decay[head]
        blocks[q, pl.ds(i, block), pl.ds(wide + i, block)] = w_input[head]
    for q in range(heads // per):
        both = dot(smoothed[:, q * wide : (q + 1) * wide], blocks[q])
        pre_r[:, q * wide : (q + 1) * wide] = both[:, :wide]
        pre_i[:, q * wide : (q + 1) * wide] = both[:, wide:]

    part0 = offset[...].astype(bf16).astype(f32)
    part1 = (offset[...] - part0).astype(bf16).astype(f32)
    part2 = offset[...] - part0 - part1
    parts = jnp.concatenate([part0, part1, part2, jnp.zeros_like(part0)], axis=0).astype(bf16)
    moved = lax.dot_general(parts, order, (((1,), (1,)), ((), ())), preferred_element_type=f32).astype(bf16)
    r = lax.broadcasted_iota(jnp.int32, (4 * heads, width), 0)
    c = lax.broadcasted_iota(jnp.int32, (4 * heads, width), 1)
    spread = jnp.where((r & (heads - 1)) == (c >> 6), -1.0, 0.0).astype(bf16)
    shift[...] = lax.dot_general(moved, spread, (((0,), (0,)), ((), ())), preferred_element_type=f32)

    rows = 4 * SUB

    def scan_rows(i, carry):
        h, p = carry
        at = pl.ds(pl.multiple_of(i * rows, rows), rows)
        retain = sigmoid(pre_r[at, :] + b_decay[...])
        admit = sigmoid(pre_i[at, :] + b_input[...])
        loss = retain * (8.0 * rate[...]) + shift[at, :]
        decay = jnp.exp(-loss)
        rest = jnp.tanh(loss) * (1.0 + decay * decay)
        drive = rest * lax.rsqrt(jnp.maximum(rest, 1e-37)) * admit * smoothed[at, :].astype(f32)
        for k in range(rows // SUB):
            a = decay[k * SUB : (k + 1) * SUB, :]
            h = a * h + drive[k * SUB : (k + 1) * SUB, :]
            p = a * p
            here = pl.ds(pl.multiple_of(i * rows + k * SUB, SUB), SUB)
            h_out[here, :] = h
            p_out[here, :] = p
        return h, p

    h, p = lax.fori_loop(
        0, length // rows, scan_rows, (jnp.zeros((SUB, width), f32), jnp.ones((SUB, width), f32))
    )
    a_before, b_before = jnp.ones((1, width), f32), jnp.zeros((1, width), f32)
    for s in range(SUB):
        runs_out[0, s : s + 1, :] = a_before
        runs_out[1, s : s + 1, :] = b_before
        a_before, b_before = a_before * p[s : s + 1, :], p[s : s + 1, :] * b_before + h[s : s + 1, :]
    pair = jnp.concatenate([a_before, b_before], axis=0)
    sent_out[...] = jnp.broadcast_to(pair[None], sent_out.shape)


def before_in(pieces, index):
    width = pieces.shape[2]
    a, b = jnp.ones((1, width), f32), jnp.zeros((1, width), f32)
    a_at, b_at = a, b
    for k in range(pieces.shape[0]):
        here = k == index
        a_at, b_at = jnp.where(here, a, a_at), jnp.where(here, b, b_at)
        a_k, b_k = pieces[k, 0:1, :], pieces[k, 1:2, :]
        a, b = a * a_k, a_k * b + b_k
    return (a_at, b_at), (a, b)


def plane_kernel(pieces, before_out, sent_out):
    index = lax.axis_index("sp_1") * lax.axis_size("sp_2") + lax.axis_index("sp_2")
    (a_at, b_at), (a, b) = before_in(pieces, index)
    before_out[...] = jnp.concatenate([a_at, b_at], axis=0)
    pair = jnp.concatenate([a, b], axis=0)
    sent_out[...] = jnp.broadcast_to(pair[None], sent_out.shape)


def state_kernel(pieces, before, runs, h, p, g, mine_out, theirs_out, gated):
    (_, b_at), _ = before_in(pieces, lax.axis_index("sp_0"))
    carried = before[0:1, :] * b_at + before[1:2, :]
    start = runs[0] * carried + runs[1]
    length = h.shape[0]
    half, run = length // 2, length // SUB
    rows = 4 * SUB
    starts = jnp.concatenate([start] * (rows // SUB), axis=0)

    def state_rows(i, _):
        at = pl.ds(pl.multiple_of(i * rows, rows), rows)
        gated[at, :] = ((h[at, :] + p[at, :] * starts) * g[at, :]).astype(bf16)
        return 0

    lax.fori_loop(0, length // rows, state_rows, 0, unroll=2)
    tp = lax.axis_index("tp")

    def back(first):
        t = lax.broadcasted_iota(jnp.int32, (half, length), 0) + first
        c = lax.broadcasted_iota(jnp.int32, (half, length), 1)
        pick = jnp.where(t == (c & (SUB - 1)) * run + (c >> 3), 1.0, 0.0).astype(bf16)
        return dot(pick, gated[...]).astype(bf16)

    theirs_out[...] = back((1 - tp) * half)
    mine_out[...] = back(tp * half)


def out_kernel(mine, theirs, w_mine, w_theirs, out, block, sent):
    cols = block.shape[2]
    copies = []
    for i in range(block.shape[0]):
        at = pl.ds(i * cols, cols)
        block[i] = (dot(mine[...], w_mine[:, at]) + dot(theirs[...], w_theirs[:, at])).astype(bf16)
        copies.append(pltpu.make_async_copy(block.at[i], out.at[:, at], sent.at[i]))
        copies[i].start()
    for copy in copies:
        copy.wait()


VMEM = pl.BlockSpec(memory_space=pltpu.VMEM)


HBM = pl.BlockSpec(memory_space=pltpu.HBM)
ARGS = 11


def call(kernel, inputs, out_shape, scratch=(), out_specs=None):
    run = pl.pallas_call(
        kernel,
        out_shape=out_shape,
        out_specs=out_specs or jax.tree.map(lambda _: VMEM, out_shape),
        scratch_shapes=list(scratch),
        compiler_params=pltpu.CompilerParams(vmem_limit_bytes=32 * 1024 * 1024),
        in_specs=[VMEM] * inputs[0] + [HBM] * inputs[1],
    )

    def place(i, a):
        return pltpu.with_memory_space_constraint(a, pltpu.VMEM if i < inputs[0] else pltpu.HBM)

    return lambda *args: run(*(place(i, a) for i, a in enumerate(args)))


def step(
    tokens,
    norm_gain,
    in_weight,
    gate_weight,
    conv_weight,
    decay_gate_weight,
    decay_gate_bias,
    input_gate_weight,
    input_gate_bias,
    channel_decay_rate,
    forgetting_offset,
    out_weight,
):
    half, features = tokens.shape
    length = 2 * half
    width = in_weight.shape[1]
    heads, block = decay_gate_weight.shape[:2]
    count = lax.axis_size(SP)
    plane = lax.axis_size(PLANE)
    deep = lax.axis_size("sp_0")
    S = jax.ShapeDtypeStruct

    swap = [(0, 1), (1, 0)]
    tail = tokens[half - HALO :]
    halo_a = lax.ppermute(tail, SP_TP, [(2 * s + 1, 2 * s + 3) for s in range(count - 1)])
    halo_b = lax.ppermute(tail, SP_TP, [(2 * s + 1, 2 * s + 2) for s in range(count - 1)])
    other = lax.ppermute(tokens, "tp", swap)
    w_theirs = lax.ppermute(out_weight, "tp", swap)

    row = lambda v: v.reshape(1, -1)
    fetched = (
        row(norm_gain), in_weight, tokens, gate_weight,
        conv_weight, decay_gate_weight, row(decay_gate_bias),
        input_gate_weight, row(input_gate_bias), row(channel_decay_rate), forgetting_offset,
    )
    big = pltpu.VMEM
    h, p, g, runs, sent = call(
        local_kernel,
        (3, ARGS),
        (
            big((length, width), f32),
            big((length, width), f32),
            big((length, width), f32),
            big((2, SUB, width), f32),
            big((plane, 2, width), f32),
        ),
        scratch=[big(a.shape, a.dtype) for i, a in enumerate(fetched) if i not in (1, 3)]
        + [
            big((features, width), bf16),
            big((features, width), bf16),
            pltpu.SemaphoreType.DMA((ARGS,)),
            big((length + 2 * HALO, features), bf16),
            big((half, 128), f32),
            big((half, 128), f32),
            big((length, width), bf16),
            big((length, width), f32),
            big((length, width), f32),
            big((length, width), f32),
            big((heads * block // 256, 256, 512), bf16),
            big((length + (conv_weight.shape[0] - 1) * SUB, width), f32),
        ],
    )(other, halo_a, halo_b, *fetched)
    pieces = lax.all_to_all(sent, PLANE, split_axis=0, concat_axis=0, tiled=True)
    before, sent = call(plane_kernel, (1, 0), (big((2, width), f32), big((deep, 2, width), f32)))(pieces)
    pieces = lax.all_to_all(sent, "sp_0", split_axis=0, concat_axis=0, tiled=True)
    mine, theirs = call(
        state_kernel,
        (6, 0),
        (big((half, width), bf16), big((half, width), bf16)),
        scratch=(big((length, width), bf16),),
    )(pieces, before, runs, h, p, g)
    received = lax.ppermute(theirs, "tp", swap)
    cols = 512
    return call(
        out_kernel,
        (4, 0),
        S((half, features), bf16),
        scratch=(big((features // cols, half, cols), bf16), pltpu.SemaphoreType.DMA((features // cols,))),
        out_specs=HBM,
    )(mine, received, out_weight, w_theirs)


def solution(mesh):
    torus = Mesh(mesh.devices.reshape(8, 8, 4, mesh.shape["tp"]), SP_TP)
    placed = (
        P(SP_TP, None),
        P(),
        P(None, "tp"),
        P(None, "tp"),
        P(None, "tp"),
        P("tp", None, None),
        P("tp"),
        P("tp", None, None),
        P("tp"),
        P("tp"),
        P("tp", SP),
        P("tp", None),
    )
    return jax.shard_map(step, mesh=torus, in_specs=placed, out_specs=P(SP_TP, None), check_vma=False)
```

```python
import jax
import jax.numpy as jnp
from jax import lax
from jax.experimental import pallas as pl
from jax.experimental.pallas import tpu as pltpu
from jax.sharding import Mesh
from jax.sharding import PartitionSpec as P

SP = ("sp_0", "sp_1", "sp_2")
PLANE = ("sp_1", "sp_2")
SP_TP = ("sp_0", "sp_1", "sp_2", "tp")

EPSILON = 1e-05
SUB = 8
HALO = 8
f32, bf16 = jnp.float32, jnp.bfloat16


def dot(a, b):
    return jnp.dot(a, b, preferred_element_type=f32)


def sigmoid(x):
    return 1.0 / (1.0 + jnp.exp(-x))


def project_kernel(other, *refs):
    stored, refs = refs[:ARGS], refs[ARGS:]
    inner, tail, normed, *held = refs[: ARGS]
    gain, w_in, own, arrived, middle, scale = refs[ARGS:]
    held = (gain, w_in, own, *held)
    copies = [pltpu.make_async_copy(a, b, arrived.at[i]) for i, (a, b) in enumerate(zip(stored, held))]
    half, features = own.shape
    tp = lax.axis_index("tp")
    step, lanes = 32, 128

    def tiles(source, r):
        return [source[r, t : t + lanes].astype(f32) for t in range(0, features, lanes)]

    def by_rows(one):
        def rows(i, _):
            one(pl.multiple_of(i * step, step))
            return 0

        lax.fori_loop(0, half // step, rows, 0)

    def over_features(stat):
        return jnp.broadcast_to(jnp.sum(stat[...], axis=1, keepdims=True) * (1.0 / features), stat.shape)

    def norm_tokens(source, base, ready=None):
        def add_up(i):
            r = pl.ds(i, step)
            middle[r, :] = sum(tiles(source, r))

        by_rows(add_up)
        middle[...] = over_features(middle)

        def add_squares(i):
            r = pl.ds(i, step)
            m = middle[r, :]
            scale[r, :] = sum((x - m) * (x - m) for x in tiles(source, r))

        by_rows(add_squares)
        scale[...] = lax.rsqrt(over_features(scale) + EPSILON)
        if ready is not None:
            ready.wait()

        def write(i):
            r = pl.ds(i, step)
            m, k = middle[r, :], scale[r, :]
            d = pl.ds(pl.multiple_of(base + i, step), step)
            for t, x in zip(range(0, features, lanes), tiles(source, r)):
                normed[d, t : t + lanes] = ((x - m) * k * gain[:, t : t + lanes]).astype(bf16)

        by_rows(write)

    for i in (0, 2, 1, *range(3, ARGS)):
        copies[i].start()
    norm_tokens(other, (1 - tp) * half, copies[0])
    copies[2].wait()
    norm_tokens(own, tp * half)
    copies[1].wait()
    both = dot(normed[...], w_in[...]).astype(bf16)
    inner[...] = both
    tail[...] = both[2 * half - HALO :]
    for copy in copies[3:]:
        copy.wait()


def gates(pre_r, pre_i, x, b_decay, b_input, rate, shift):
    retain = sigmoid(pre_r + b_decay)
    admit = sigmoid(pre_i + b_input)
    loss = retain * (8.0 * rate) + shift
    decay = jnp.exp(-loss)
    rest = jnp.tanh(loss) * (1.0 + decay * decay)
    return decay, rest * lax.rsqrt(jnp.maximum(rest, 1e-37)) * admit * x


def block_dots(smoothed, blocks, store):
    wide = blocks.shape[1]
    for q in range(blocks.shape[0]):
        at = slice(q * wide, (q + 1) * wide)
        both = dot(smoothed[:, at], blocks[q])
        store(at, both[:, :wide], both[:, wide:])


def scan_kernel(
    inner, normed, w_gate, conv, w_decay, b_decay, w_input, b_input, rate, offset,
    h_out, p_out, g_out, ends_out, blocks, heads_shift,
    smoothed, pre_r, pre_i, shift, extended,
):
    length, width = inner.shape
    run = length // SUB
    taps = conv.shape[0]
    lead = (taps - 1) * SUB

    def picks(rows, base):
        r = lax.broadcasted_iota(jnp.int32, (rows, length), 0)
        c = lax.broadcasted_iota(jnp.int32, (rows, length), 1)
        return jnp.where(c == (r & (SUB - 1)) * run + (r >> 3) + base, 1.0, 0.0).astype(bf16)

    order = picks(length, 0)
    extended[pl.ds(lead, length), :] = dot(order, inner[...])
    extended[pl.ds(0, lead), :] = dot(picks(lead, 1 - taps), inner[...])
    gate = dot(normed[...], w_gate[...]).astype(bf16)
    g_out[...] = jax.nn.gelu(dot(order, gate))

    smooth = extended[pl.ds(0, length), :] * conv[0:1, :]
    for tap in range(1, taps):
        smooth = smooth + extended[pl.ds(tap * SUB, length), :] * conv[tap : tap + 1, :]
    smoothed[...] = smooth.astype(bf16)

    heads, block = w_decay.shape[0], w_decay.shape[1]
    wide = blocks.shape[1]
    per = wide // block
    blocks[...] = jnp.zeros_like(blocks)
    for head in range(heads):
        q, i = head // per, (head % per) * block
        blocks[q, pl.ds(i, block), pl.ds(i, block)] = w_decay[head]
        blocks[q, pl.ds(i, block), pl.ds(wide + i, block)] = w_input[head]

    def store(at, r, i):
        pre_r[:, at] = r
        pre_i[:, at] = i

    block_dots(smoothed, blocks, store)

    part0 = offset[...].astype(bf16).astype(f32)
    part1 = (offset[...] - part0).astype(bf16).astype(f32)
    part2 = offset[...] - part0 - part1
    parts = jnp.concatenate([part0, part1, part2, jnp.zeros_like(part0)], axis=0).astype(bf16)
    moved = lax.dot_general(parts, order, (((1,), (1,)), ((), ())), preferred_element_type=f32).astype(bf16)
    r = lax.broadcasted_iota(jnp.int32, (4 * heads, width), 0)
    c = lax.broadcasted_iota(jnp.int32, (4 * heads, width), 1)
    spread = jnp.where((r & (heads - 1)) == (c >> 6), -1.0, 0.0).astype(bf16)
    shift[...] = lax.dot_general(moved, spread, (((0,), (0,)), ((), ())), preferred_element_type=f32)
    heads_shift[...] = shift[pl.ds(0, heads_shift.shape[0]), :]

    rows = 4 * SUB

    def scan_rows(i, carry, skip=0):
        h, p = carry
        at = pl.ds(pl.multiple_of(i * rows, rows), rows)
        decay, drive = gates(
            pre_r[at, :], pre_i[at, :], smoothed[at, :].astype(f32), b_decay[...], b_input[...], rate[...], shift[at, :]
        )
        known = lax.broadcasted_iota(jnp.int32, (SUB, width), 0) > 0
        for k in range(rows // SUB):
            a, b = decay[k * SUB : (k + 1) * SUB, :], drive[k * SUB : (k + 1) * SUB, :]
            if k < skip:
                a, b = jnp.where(known, a, 1.0), jnp.where(known, b, 0.0)
            h = a * h + b
            p = a * p
            here = pl.ds(pl.multiple_of(i * rows + k * SUB, SUB), SUB)
            h_out[here, :] = h
            p_out[here, :] = p
        return h, p

    start = (jnp.zeros((SUB, width), f32), jnp.ones((SUB, width), f32))
    h, p = lax.fori_loop(1, length // rows, scan_rows, scan_rows(0, start, taps - 1))
    ends_out[0] = p
    ends_out[1] = h


def head_kernel(
    inner, halo, conv, blocks, b_decay, b_input, rate, shift, ends,
    runs_out, heads_out, sent_out,
    near, smoothed, pre_r, pre_i,
):
    width = inner.shape[1]
    taps = conv.shape[0]
    near[pl.ds(0, HALO), :] = halo[...].astype(f32)
    near[pl.ds(HALO, HALO), :] = inner[pl.ds(0, 2 * HALO), :].astype(f32)[:HALO]
    smooth = near[pl.ds(HALO - taps + 1, HALO), :] * conv[0:1, :]
    for tap in range(1, taps):
        smooth = smooth + near[pl.ds(HALO - taps + 1 + tap, HALO), :] * conv[tap : tap + 1, :]
    smoothed[...] = jnp.concatenate([smooth, jnp.zeros_like(smooth)], axis=0).astype(bf16)

    def store(at, r, i):
        pre_r[:, at] = r[:HALO]
        pre_i[:, at] = i[:HALO]

    block_dots(smoothed, blocks, store)
    shifts = jnp.concatenate([shift[pl.ds(k * SUB, 1), :] for k in range(HALO)], axis=0)
    decay, drive = gates(
        pre_r[...], pre_i[...], smoothed[...].astype(f32)[:HALO], b_decay[...], b_input[...], rate[...], shifts
    )
    a_before, b_before = jnp.ones((1, width), f32), jnp.zeros((1, width), f32)
    for k in range(taps - 1):
        a_k = decay[k : k + 1, :]
        a_before, b_before = a_before * a_k, a_k * b_before + drive[k : k + 1, :]
        heads_out[0, k : k + 1, :] = a_before
        heads_out[1, k : k + 1, :] = b_before
    for s in range(SUB):
        runs_out[0, s : s + 1, :] = a_before
        runs_out[1, s : s + 1, :] = b_before
        a_s = ends[0, s : s + 1, :]
        a_before, b_before = a_before * a_s, a_s * b_before + ends[1, s : s + 1, :]
    pair = jnp.concatenate([a_before, b_before], axis=0)
    sent_out[...] = jnp.broadcast_to(pair[None], sent_out.shape)


def before_in(pieces, index):
    width = pieces.shape[2]
    a, b = jnp.ones((1, width), f32), jnp.zeros((1, width), f32)
    a_at, b_at = a, b
    for k in range(pieces.shape[0]):
        here = k == index
        a_at, b_at = jnp.where(here, a, a_at), jnp.where(here, b, b_at)
        a_k, b_k = pieces[k, 0:1, :], pieces[k, 1:2, :]
        a, b = a * a_k, a_k * b + b_k
    return (a_at, b_at), (a, b)


def plane_kernel(pieces, before_out, sent_out):
    index = lax.axis_index("sp_1") * lax.axis_size("sp_2") + lax.axis_index("sp_2")
    (a_at, b_at), (a, b) = before_in(pieces, index)
    before_out[...] = jnp.concatenate([a_at, b_at], axis=0)
    pair = jnp.concatenate([a, b], axis=0)
    sent_out[...] = jnp.broadcast_to(pair[None], sent_out.shape)


def back(gated, first):
    length = gated.shape[0]
    half, run = length // 2, length // SUB
    t = lax.broadcasted_iota(jnp.int32, (half, length), 0) + first
    c = lax.broadcasted_iota(jnp.int32, (half, length), 1)
    pick = jnp.where(t == (c & (SUB - 1)) * run + (c >> 3), 1.0, 0.0).astype(bf16)
    return dot(pick, gated[...]).astype(bf16)


def state_kernel(pieces, before, runs, heads, h, p, g, gated, theirs_out):
    (_, b_at), _ = before_in(pieces, lax.axis_index("sp_0"))
    carried = before[0:1, :] * b_at + before[1:2, :]
    start = runs[0] * carried + runs[1]
    length = h.shape[0]
    rows = 4 * SUB
    opening = heads[0] * carried + heads[1]
    first = [jnp.concatenate([opening[k : k + 1], start[1:]], axis=0) for k in range(heads.shape[1])]
    groups = rows // SUB

    def state_rows(i, starts):
        at = pl.ds(pl.multiple_of(i * rows, rows), rows)
        gated[at, :] = ((h[at, :] + p[at, :] * starts) * g[at, :]).astype(bf16)
        return starts

    state_rows(0, jnp.concatenate(first + [start] * (groups - len(first)), axis=0))
    starts = jnp.concatenate([start] * groups, axis=0)
    lax.fori_loop(1, length // rows, lambda i, _: (state_rows(i, starts), 0)[1], 0)
    theirs_out[...] = back(gated, (1 - lax.axis_index("tp")) * (length // 2))


def own_kernel(gated, w_mine, part):
    mine = back(gated, lax.axis_index("tp") * (gated.shape[0] // 2))
    part[...] = dot(mine, w_mine[...])


def out_kernel(part, theirs, w_theirs, out, block, sent):
    cols = block.shape[2]
    copies = []
    for i in range(block.shape[0]):
        at = pl.ds(i * cols, cols)
        block[i] = (part[:, at] + dot(theirs[...], w_theirs[:, at])).astype(bf16)
        copies.append(pltpu.make_async_copy(block.at[i], out.at[:, at], sent.at[i]))
        copies[i].start()
    for copy in copies:
        copy.wait()


VMEM = pl.BlockSpec(memory_space=pltpu.VMEM)


HBM = pl.BlockSpec(memory_space=pltpu.HBM)
ARGS = 11


def call(kernel, inputs, out_shape, scratch=(), out_specs=None):
    run = pl.pallas_call(
        kernel,
        out_shape=out_shape,
        out_specs=out_specs or jax.tree.map(lambda _: VMEM, out_shape),
        scratch_shapes=list(scratch),
        compiler_params=pltpu.CompilerParams(vmem_limit_bytes=32 * 1024 * 1024),
        in_specs=[VMEM] * inputs[0] + [HBM] * inputs[1],
    )

    def place(i, a):
        return pltpu.with_memory_space_constraint(a, pltpu.VMEM if i < inputs[0] else pltpu.HBM)

    return lambda *args: run(*(place(i, a) for i, a in enumerate(args)))


def step(
    tokens,
    norm_gain,
    in_weight,
    gate_weight,
    conv_weight,
    decay_gate_weight,
    decay_gate_bias,
    input_gate_weight,
    input_gate_bias,
    channel_decay_rate,
    forgetting_offset,
    out_weight,
):
    half, features = tokens.shape
    length = 2 * half
    width = in_weight.shape[1]
    heads, block = decay_gate_weight.shape[:2]
    count = lax.axis_size(SP)
    plane = lax.axis_size(PLANE)
    deep = lax.axis_size("sp_0")
    S = jax.ShapeDtypeStruct

    swap = [(0, 1), (1, 0)]
    other = lax.ppermute(tokens, "tp", swap)
    w_theirs = lax.ppermute(out_weight, "tp", swap)

    row = lambda v: v.reshape(1, -1)
    fetched = (
        row(norm_gain), in_weight, tokens, gate_weight,
        conv_weight, decay_gate_weight, row(decay_gate_bias),
        input_gate_weight, row(input_gate_bias), row(channel_decay_rate), forgetting_offset,
    )
    big = pltpu.VMEM
    like = lambda a: big(a.shape, a.dtype)
    square = big((length, width), f32)
    inner, tail, normed, *held = call(
        project_kernel,
        (1, ARGS),
        (
            big((length, width), bf16), big((HALO, width), bf16), big((length, features), bf16),
            *(like(a) for a in fetched[3:]),
        ),
        scratch=[
            *(like(a) for a in fetched[:3]),
            pltpu.SemaphoreType.DMA((ARGS,)),
            big((half, 128), f32),
            big((half, 128), f32),
        ],
    )(other, *fetched)
    w_gate, conv, w_decay, b_decay, w_input, b_input, rate, offset = held
    halo = lax.ppermute(tail, SP, [(s, s + 1) for s in range(count - 1)])
    taps = conv_weight.shape[0]
    h, p, g, ends, blocks, shift = call(
        scan_kernel,
        (10, 0),
        (
            square, square, square, big((2, SUB, width), f32),
            big((heads * block // 256, 256, 512), bf16), big((HALO * SUB, width), f32),
        ),
        scratch=[
            big((length, width), bf16), square, square, square,
            big((length + (taps - 1) * SUB, width), f32),
        ],
    )(inner, normed, w_gate, conv, w_decay, b_decay, w_input, b_input, rate, offset)
    runs, opening, sent = call(
        head_kernel,
        (9, 0),
        (big((2, SUB, width), f32), big((2, taps - 1, width), f32), big((plane, 2, width), f32)),
        scratch=[
            big((2 * HALO, width), f32), big((2 * HALO, width), bf16),
            big((HALO, width), f32), big((HALO, width), f32),
        ],
    )(inner, halo, conv, blocks, b_decay, b_input, rate, shift, ends)
    pieces = lax.all_to_all(sent, PLANE, split_axis=0, concat_axis=0, tiled=True)
    before, sent = call(plane_kernel, (1, 0), (big((2, width), f32), big((deep, 2, width), f32)))(pieces)
    pieces = lax.all_to_all(sent, "sp_0", split_axis=0, concat_axis=0, tiled=True)
    gated, theirs = call(
        state_kernel, (7, 0), (big((length, width), bf16), big((half, width), bf16))
    )(pieces, before, runs, opening, h, p, g)
    received = lax.ppermute(theirs, "tp", swap)
    part = call(own_kernel, (2, 0), big((half, features), f32))(gated, out_weight)
    cols = 512
    return call(
        out_kernel,
        (3, 0),
        S((half, features), bf16),
        scratch=(big((features // cols, half, cols), bf16), pltpu.SemaphoreType.DMA((features // cols,))),
        out_specs=HBM,
    )(part, received, w_theirs)


def solution(mesh):
    torus = Mesh(mesh.devices.reshape(8, 8, 4, mesh.shape["tp"]), SP_TP)
    placed = (
        P(SP_TP, None),
        P(),
        P(None, "tp"),
        P(None, "tp"),
        P(None, "tp"),
        P("tp", None, None),
        P("tp"),
        P("tp", None, None),
        P("tp"),
        P("tp"),
        P("tp", SP),
        P("tp", None),
    )
    return jax.shard_map(step, mesh=torus, in_specs=placed, out_specs=P(SP_TP, None), check_vma=False)
```

```python
import jax
import jax.numpy as jnp
from jax import lax
from jax.experimental import pallas as pl
from jax.experimental.pallas import tpu as pltpu
from jax.sharding import Mesh
from jax.sharding import PartitionSpec as P

SP = ("sp_0", "sp_1", "sp_2")
PLANE = ("sp_1", "sp_2")
SP_TP = ("sp_0", "sp_1", "sp_2", "tp")

EPSILON = 1e-05
SUB = 8
HALO = 8
f32, bf16 = jnp.float32, jnp.bfloat16


def dot(a, b):
    return jnp.dot(a, b, preferred_element_type=f32)


def sigmoid(x):
    return 1.0 / (1.0 + jnp.exp(-x))


def norm_tokens(source, target, gain, middle, scale, ready=None):
    half, features = source.shape
    step, lanes = 32, 128

    def tiles(r):
        return [source[r, t : t + lanes].astype(f32) for t in range(0, features, lanes)]

    def by_rows(one):
        def rows(i, _):
            one(pl.ds(pl.multiple_of(i * step, step), step))
            return 0

        lax.fori_loop(0, half // step, rows, 0)

    def over_features(stat):
        return jnp.broadcast_to(jnp.sum(stat[...], axis=1, keepdims=True) * (1.0 / features), stat.shape)

    def add_up(r):
        middle[r, :] = sum(tiles(r))

    by_rows(add_up)
    middle[...] = over_features(middle)

    def add_squares(r):
        m = middle[r, :]
        scale[r, :] = sum((x - m) * (x - m) for x in tiles(r))

    by_rows(add_squares)
    scale[...] = lax.rsqrt(over_features(scale) + EPSILON)
    if ready is not None:
        ready.wait()

    def write(r):
        m, k = middle[r, :], scale[r, :]
        for t, x in zip(range(0, features, lanes), tiles(r)):
            target[r, t : t + lanes] = ((x - m) * k * gain[:, t : t + lanes]).astype(bf16)

    by_rows(write)


def own_tokens_kernel(*refs):
    stored, refs = refs[:ARGS], refs[ARGS:]
    inner, normed, *held = refs[: ARGS + 1]
    own, arrived, middle, scale = refs[ARGS + 1 :]
    held.insert(2, own)
    gain, w_in = held[:2]
    copies = [pltpu.make_async_copy(a, b, arrived.at[i]) for i, (a, b) in enumerate(zip(stored, held))]
    for i in (2, 0, 1, *range(3, ARGS)):
        copies[i].start()
    copies[2].wait()
    norm_tokens(own, normed, gain, middle, scale, copies[0])
    copies[1].wait()
    inner[...] = dot(normed[...], w_in[...]).astype(bf16)
    for copy in copies[3:]:
        copy.wait()


def other_tokens_kernel(other, gain, w_in, inner_own, inner, tail, normed, middle, scale):
    half = other.shape[0]
    tp = lax.axis_index("tp")
    norm_tokens(other, normed, gain, middle, scale)
    inner[pl.ds(pl.multiple_of(tp * half, half), half), :] = inner_own[...]
    there = pl.ds(pl.multiple_of((1 - tp) * half, half), half)
    inner[there, :] = dot(normed[...], w_in[...]).astype(bf16)
    tail[...] = inner[pl.ds(2 * half - 2 * HALO, 2 * HALO), :].astype(f32)[HALO:].astype(bf16)


def gates(pre_r, pre_i, x, b_decay, b_input, rate, shift):
    retain = sigmoid(pre_r + b_decay)
    admit = sigmoid(pre_i + b_input)
    loss = retain * (8.0 * rate) + shift
    decay = jnp.exp(-loss)
    rest = jnp.tanh(loss) * (1.0 + decay * decay)
    return decay, rest * lax.rsqrt(jnp.maximum(rest, 1e-37)) * admit * x


def block_dots(smoothed, blocks, store):
    wide = blocks.shape[1]
    for q in range(blocks.shape[0]):
        at = slice(q * wide, (q + 1) * wide)
        both = dot(smoothed[:, at], blocks[q])
        store(at, both[:, :wide], both[:, wide:])


def scan_kernel(
    inner, normed_own, normed_other, w_gate, conv, w_decay, b_decay, w_input, b_input, rate, offset,
    h_out, p_out, g_out, ends_out, blocks, heads_shift,
    smoothed, pre_r, pre_i, shift, extended, gate,
):
    length, width = inner.shape
    run = length // SUB
    taps = conv.shape[0]
    lead = (taps - 1) * SUB

    def picks(rows, base):
        r = lax.broadcasted_iota(jnp.int32, (rows, length), 0)
        c = lax.broadcasted_iota(jnp.int32, (rows, length), 1)
        return jnp.where(c == (r & (SUB - 1)) * run + (r >> 3) + base, 1.0, 0.0).astype(bf16)

    order = picks(length, 0)
    extended[pl.ds(lead, length), :] = dot(order, inner[...])
    extended[pl.ds(0, lead), :] = dot(picks(lead, 1 - taps), inner[...])

    smooth = extended[pl.ds(0, length), :] * conv[0:1, :]
    for tap in range(1, taps):
        smooth = smooth + extended[pl.ds(tap * SUB, length), :] * conv[tap : tap + 1, :]
    smoothed[...] = smooth.astype(bf16)

    heads, block = w_decay.shape[0], w_decay.shape[1]
    wide = blocks.shape[1]
    per = wide // block
    blocks[...] = jnp.zeros_like(blocks)
    for head in range(heads):
        q, i = head // per, (head % per) * block
        blocks[q, pl.ds(i, block), pl.ds(i, block)] = w_decay[head]
        blocks[q, pl.ds(i, block), pl.ds(wide + i, block)] = w_input[head]

    def store(at, r, i):
        pre_r[:, at] = r
        pre_i[:, at] = i

    block_dots(smoothed, blocks, store)

    part0 = offset[...].astype(bf16).astype(f32)
    part1 = (offset[...] - part0).astype(bf16).astype(f32)
    part2 = offset[...] - part0 - part1
    parts = jnp.concatenate([part0, part1, part2, jnp.zeros_like(part0)], axis=0).astype(bf16)
    moved = lax.dot_general(parts, order, (((1,), (1,)), ((), ())), preferred_element_type=f32).astype(bf16)
    r = lax.broadcasted_iota(jnp.int32, (4 * heads, width), 0)
    c = lax.broadcasted_iota(jnp.int32, (4 * heads, width), 1)
    spread = jnp.where((r & (heads - 1)) == (c >> 6), -1.0, 0.0).astype(bf16)
    shift[...] = lax.dot_general(moved, spread, (((0,), (0,)), ((), ())), preferred_element_type=f32)
    heads_shift[...] = shift[pl.ds(0, heads_shift.shape[0]), :]

    rows = 4 * SUB

    def scan_rows(i, carry, skip=0):
        h, p = carry
        at = pl.ds(pl.multiple_of(i * rows, rows), rows)
        decay, drive = gates(
            pre_r[at, :], pre_i[at, :], smoothed[at, :].astype(f32), b_decay[...], b_input[...], rate[...], shift[at, :]
        )
        known = lax.broadcasted_iota(jnp.int32, (SUB, width), 0) > 0
        for k in range(rows // SUB):
            a, b = decay[k * SUB : (k + 1) * SUB, :], drive[k * SUB : (k + 1) * SUB, :]
            if k < skip:
                a, b = jnp.where(known, a, 1.0), jnp.where(known, b, 0.0)
            h = a * h + b
            p = a * p
            here = pl.ds(pl.multiple_of(i * rows + k * SUB, SUB), SUB)
            h_out[here, :] = h
            p_out[here, :] = p
        return h, p

    start = (jnp.zeros((SUB, width), f32), jnp.ones((SUB, width), f32))
    h, p = start
    half, blocks_half = length // 2, length // rows // 2
    tp = lax.axis_index("tp")
    for c, (normed, place) in enumerate(((normed_own, tp), (normed_other, 1 - tp))):
        at = pl.ds(pl.multiple_of(place * half, half), half)
        gate[at, :] = dot(normed[...], w_gate[...]).astype(bf16)
        for i in range(c * blocks_half, (c + 1) * blocks_half):
            h, p = scan_rows(i, (h, p), 0 if i else taps - 1)
    g_out[...] = jax.nn.gelu(dot(order, gate[...]))
    ends_out[0] = p
    ends_out[1] = h


def head_kernel(
    inner, halo, conv, blocks, b_decay, b_input, rate, shift, ends,
    runs_out, heads_out, sent_out,
    near, smoothed, pre_r, pre_i,
):
    width = inner.shape[1]
    taps = conv.shape[0]
    near[pl.ds(0, HALO), :] = halo[...].astype(f32)
    near[pl.ds(HALO, HALO), :] = inner[pl.ds(0, 2 * HALO), :].astype(f32)[:HALO]
    smooth = near[pl.ds(HALO - taps + 1, HALO), :] * conv[0:1, :]
    for tap in range(1, taps):
        smooth = smooth + near[pl.ds(HALO - taps + 1 + tap, HALO), :] * conv[tap : tap + 1, :]
    smoothed[...] = jnp.concatenate([smooth, jnp.zeros_like(smooth)], axis=0).astype(bf16)

    def store(at, r, i):
        pre_r[:, at] = r[:HALO]
        pre_i[:, at] = i[:HALO]

    block_dots(smoothed, blocks, store)
    shifts = jnp.concatenate([shift[pl.ds(k * SUB, 1), :] for k in range(HALO)], axis=0)
    decay, drive = gates(
        pre_r[...], pre_i[...], smoothed[...].astype(f32)[:HALO], b_decay[...], b_input[...], rate[...], shifts
    )
    a_before, b_before = jnp.ones((1, width), f32), jnp.zeros((1, width), f32)
    for k in range(taps - 1):
        a_k = decay[k : k + 1, :]
        a_before, b_before = a_before * a_k, a_k * b_before + drive[k : k + 1, :]
        heads_out[0, k : k + 1, :] = a_before
        heads_out[1, k : k + 1, :] = b_before
    for s in range(SUB):
        runs_out[0, s : s + 1, :] = a_before
        runs_out[1, s : s + 1, :] = b_before
        a_s = ends[0, s : s + 1, :]
        a_before, b_before = a_before * a_s, a_s * b_before + ends[1, s : s + 1, :]
    pair = jnp.concatenate([a_before, b_before], axis=0)
    sent_out[...] = jnp.broadcast_to(pair[None], sent_out.shape)


def before_in(pieces, index):
    width = pieces.shape[2]
    a, b = jnp.ones((1, width), f32), jnp.zeros((1, width), f32)
    a_at, b_at = a, b
    for k in range(pieces.shape[0]):
        here = k == index
        a_at, b_at = jnp.where(here, a, a_at), jnp.where(here, b, b_at)
        a_k, b_k = pieces[k, 0:1, :], pieces[k, 1:2, :]
        a, b = a * a_k, a_k * b + b_k
    return (a_at, b_at), (a, b)


def plane_kernel(pieces, before_out, sent_out):
    index = lax.axis_index("sp_1") * lax.axis_size("sp_2") + lax.axis_index("sp_2")
    (a_at, b_at), (a, b) = before_in(pieces, index)
    before_out[...] = jnp.concatenate([a_at, b_at], axis=0)
    pair = jnp.concatenate([a, b], axis=0)
    sent_out[...] = jnp.broadcast_to(pair[None], sent_out.shape)


def back(gated, first):
    length = gated.shape[0]
    half, run = length // 2, length // SUB
    t = lax.broadcasted_iota(jnp.int32, (half, length), 0) + first
    c = lax.broadcasted_iota(jnp.int32, (half, length), 1)
    pick = jnp.where(t == (c & (SUB - 1)) * run + (c >> 3), 1.0, 0.0).astype(bf16)
    return dot(pick, gated[...]).astype(bf16)


def state_kernel(pieces, before, runs, heads, h, p, g, w_mine, gated, theirs_out):
    (_, b_at), _ = before_in(pieces, lax.axis_index("sp_0"))
    carried = before[0:1, :] * b_at + before[1:2, :]
    start = runs[0] * carried + runs[1]
    length = h.shape[0]
    rows = 4 * SUB
    opening = heads[0] * carried + heads[1]
    first = [jnp.concatenate([opening[k : k + 1], start[1:]], axis=0) for k in range(heads.shape[1])]
    groups = rows // SUB

    def state_rows(i, starts):
        at = pl.ds(pl.multiple_of(i * rows, rows), rows)
        gated[at, :] = ((h[at, :] + p[at, :] * starts) * g[at, :]).astype(bf16)
        return starts

    state_rows(0, jnp.concatenate(first + [start] * (groups - len(first)), axis=0))
    starts = jnp.concatenate([start] * groups, axis=0)
    lax.fori_loop(1, length // rows, lambda i, _: (state_rows(i, starts), 0)[1], 0)
    theirs = back(gated, (1 - lax.axis_index("tp")) * (length // 2))
    theirs_out[...] = dot(theirs, w_mine[...]).astype(bf16)


def own_kernel(gated, w_mine, part):
    mine = back(gated, lax.axis_index("tp") * (gated.shape[0] // 2))
    part[...] = dot(mine, w_mine[...])


def out_kernel(part, received, out, block, sent):
    rows = block.shape[1]
    copies = []
    for i in range(block.shape[0]):
        at = pl.ds(i * rows, rows)
        block[i] = (part[at, :] + received[at, :].astype(f32)).astype(bf16)
        copies.append(pltpu.make_async_copy(block.at[i], out.at[at, :], sent.at[i]))
        copies[i].start()
    for copy in copies:
        copy.wait()


VMEM = pl.BlockSpec(memory_space=pltpu.VMEM)


HBM = pl.BlockSpec(memory_space=pltpu.HBM)
ARGS = 11


def call(kernel, inputs, out_shape, scratch=(), out_specs=None):
    run = pl.pallas_call(
        kernel,
        out_shape=out_shape,
        out_specs=out_specs or jax.tree.map(lambda _: VMEM, out_shape),
        scratch_shapes=list(scratch),
        compiler_params=pltpu.CompilerParams(vmem_limit_bytes=32 * 1024 * 1024),
        in_specs=[VMEM] * inputs[0] + [HBM] * inputs[1],
    )

    def place(i, a):
        return pltpu.with_memory_space_constraint(a, pltpu.VMEM if i < inputs[0] else pltpu.HBM)

    return lambda *args: run(*(place(i, a) for i, a in enumerate(args)))


def step(
    tokens,
    norm_gain,
    in_weight,
    gate_weight,
    conv_weight,
    decay_gate_weight,
    decay_gate_bias,
    input_gate_weight,
    input_gate_bias,
    channel_decay_rate,
    forgetting_offset,
    out_weight,
):
    half, features = tokens.shape
    length = 2 * half
    width = in_weight.shape[1]
    heads, block = decay_gate_weight.shape[:2]
    count = lax.axis_size(SP)
    plane = lax.axis_size(PLANE)
    deep = lax.axis_size("sp_0")
    S = jax.ShapeDtypeStruct

    swap = [(0, 1), (1, 0)]
    other = lax.ppermute(tokens, "tp", swap)

    row = lambda v: v.reshape(1, -1)
    fetched = (
        row(norm_gain), in_weight, tokens, gate_weight,
        conv_weight, decay_gate_weight, row(decay_gate_bias),
        input_gate_weight, row(input_gate_bias), row(channel_decay_rate), forgetting_offset,
    )
    big = pltpu.VMEM
    like = lambda a: big(a.shape, a.dtype)
    square = big((length, width), f32)
    stats = [big((half, 128), f32), big((half, 128), f32)]
    inner_own, normed_own, gain, w_in, *held = call(
        own_tokens_kernel,
        (0, ARGS),
        (
            big((half, width), bf16), big((half, features), bf16),
            *(like(a) for i, a in enumerate(fetched) if i != 2),
        ),
        scratch=[like(tokens), pltpu.SemaphoreType.DMA((ARGS,)), *stats],
    )(*fetched)
    inner, tail, normed_other = call(
        other_tokens_kernel,
        (4, 0),
        (big((length, width), bf16), big((HALO, width), bf16), big((half, features), bf16)),
        scratch=stats,
    )(other, gain, w_in, inner_own)
    w_gate, conv, w_decay, b_decay, w_input, b_input, rate, offset = held
    halo = lax.ppermute(tail, SP, [(s, s + 1) for s in range(count - 1)])
    taps = conv_weight.shape[0]
    h, p, g, ends, blocks, shift = call(
        scan_kernel,
        (11, 0),
        (
            square, square, square, big((2, SUB, width), f32),
            big((heads * block // 256, 256, 512), bf16), big((HALO * SUB, width), f32),
        ),
        scratch=[
            big((length, width), bf16), square, square, square,
            big((length + (taps - 1) * SUB, width), f32), big((length, width), bf16),
        ],
    )(inner, normed_own, normed_other, w_gate, conv, w_decay, b_decay, w_input, b_input, rate, offset)
    runs, opening, sent = call(
        head_kernel,
        (9, 0),
        (big((2, SUB, width), f32), big((2, taps - 1, width), f32), big((plane, 2, width), f32)),
        scratch=[
            big((2 * HALO, width), f32), big((2 * HALO, width), bf16),
            big((HALO, width), f32), big((HALO, width), f32),
        ],
    )(inner, halo, conv, blocks, b_decay, b_input, rate, shift, ends)
    pieces = lax.all_to_all(sent, PLANE, split_axis=0, concat_axis=0, tiled=True)
    before, sent = call(plane_kernel, (1, 0), (big((2, width), f32), big((deep, 2, width), f32)))(pieces)
    pieces = lax.all_to_all(sent, "sp_0", split_axis=0, concat_axis=0, tiled=True)
    gated, theirs = call(
        state_kernel, (8, 0), (big((length, width), bf16), big((half, features), bf16))
    )(pieces, before, runs, opening, h, p, g, out_weight)
    received = lax.ppermute(theirs, "tp", swap)
    part = call(own_kernel, (2, 0), big((half, features), f32))(gated, out_weight)
    rows = 64
    return call(
        out_kernel,
        (2, 0),
        S((half, features), bf16),
        scratch=(big((half // rows, rows, features), bf16), pltpu.SemaphoreType.DMA((half // rows,))),
        out_specs=HBM,
    )(part, received)


def solution(mesh):
    torus = Mesh(mesh.devices.reshape(8, 8, 4, mesh.shape["tp"]), SP_TP)
    placed = (
        P(SP_TP, None),
        P(),
        P(None, "tp"),
        P(None, "tp"),
        P(None, "tp"),
        P("tp", None, None),
        P("tp"),
        P("tp", None, None),
        P("tp"),
        P("tp"),
        P("tp", SP),
        P("tp", None),
    )
    return jax.shard_map(step, mesh=torus, in_specs=placed, out_specs=P(SP_TP, None), check_vma=False)
```

```python
import jax
import jax.numpy as jnp
from jax import lax
from jax.experimental import pallas as pl
from jax.experimental.pallas import tpu as pltpu
from jax.sharding import Mesh
from jax.sharding import PartitionSpec as P

SP = ("sp_0", "sp_1", "sp_2")
PLANE = ("sp_1", "sp_2")
SP_TP = ("sp_0", "sp_1", "sp_2", "tp")

EPSILON = 1e-05
SUB = 8
HALO = 8
f32, bf16 = jnp.float32, jnp.bfloat16


def dot(a, b):
    return jnp.dot(a, b, preferred_element_type=f32)


def norm_tokens(source, target, gain, middle, scale, ready=None):
    half, features = source.shape
    step, lanes = 32, 128

    def tiles(r):
        return [source[r, t : t + lanes].astype(f32) for t in range(0, features, lanes)]

    def by_rows(one):
        def rows(i, _):
            one(pl.ds(pl.multiple_of(i * step, step), step))
            return 0

        lax.fori_loop(0, half // step, rows, 0)

    def over_features(stat):
        return jnp.broadcast_to(jnp.sum(stat[...], axis=1, keepdims=True) * (1.0 / features), stat.shape)

    def add_up(r):
        middle[r, :] = sum(tiles(r))

    by_rows(add_up)
    middle[...] = over_features(middle)

    def add_squares(r):
        m = middle[r, :]
        scale[r, :] = sum((x - m) * (x - m) for x in tiles(r))

    by_rows(add_squares)
    scale[...] = lax.rsqrt(over_features(scale) + EPSILON)
    if ready is not None:
        ready.wait()

    def write(r):
        m, k = middle[r, :], scale[r, :]
        for t, x in zip(range(0, features, lanes), tiles(r)):
            target[r, t : t + lanes] = ((x - m) * k * gain[:, t : t + lanes]).astype(bf16)

    by_rows(write)


def fetch(stored, held, arrived, order):
    copies = [pltpu.make_async_copy(a, b, arrived.at[i]) for i, (a, b) in enumerate(zip(stored, held))]
    for i in order:
        copies[i].start()
    return copies


def own_tokens_kernel(gain_in, w_in_in, own_in, inner, normed, gain, w_in, own, arrived, middle, scale):
    copies = fetch((gain_in, w_in_in, own_in), (gain, w_in, own), arrived, (2, 0, 1))
    copies[2].wait()
    norm_tokens(own, normed, gain, middle, scale, copies[0])
    copies[1].wait()
    inner[...] = dot(normed[...], w_in[...]).astype(bf16)


def other_tokens_kernel(other, gain, w_in, inner_own, *refs):
    stored, refs = refs[:LATER], refs[LATER:]
    inner, tail, normed, *held = refs[: 3 + LATER]
    arrived, middle, scale = refs[3 + LATER :]
    copies = fetch(stored, held, arrived, range(LATER))
    half = other.shape[0]
    tp = lax.axis_index("tp")
    norm_tokens(other, normed, gain, middle, scale)
    inner[pl.ds(pl.multiple_of(tp * half, half), half), :] = inner_own[...]
    there = pl.ds(pl.multiple_of((1 - tp) * half, half), half)
    inner[there, :] = dot(normed[...], w_in[...]).astype(bf16)
    tail[...] = inner[pl.ds(2 * half - 2 * HALO, 2 * HALO), :].astype(f32)[HALO:].astype(bf16)
    for copy in copies:
        copy.wait()


def gates(minus_r, minus_i, x, b_decay, b_input, rate, shift):
    retain = 1.0 / (1.0 + jnp.exp(minus_r - b_decay))
    admit = 1.0 / (1.0 + jnp.exp(minus_i - b_input))
    log_decay = retain * (-8.0 * rate) + shift
    decay = jnp.exp(log_decay)
    rest = jnp.tanh(log_decay) * (-1.0 - decay * decay)
    return decay, rest * lax.rsqrt(jnp.maximum(rest, 1e-37)) * admit * x


def block_dots(smoothed, blocks, store):
    wide = blocks.shape[1]
    for q in range(blocks.shape[0]):
        at = slice(q * wide, (q + 1) * wide)
        both = dot(smoothed[:, at], blocks[q])
        store(at, both[:, :wide], both[:, wide:])


def scan_kernel(
    inner, normed_own, normed_other, w_gate, conv, w_decay, b_decay, w_input, b_input, rate, offset,
    h_out, p_out, g_out, ends_out, blocks, heads_shift,
    smoothed, pre_r, pre_i, shift, extended, gate,
):
    length, width = inner.shape
    run = length // SUB
    taps = conv.shape[0]
    lead = (taps - 1) * SUB

    def picks(rows, base):
        r = lax.broadcasted_iota(jnp.int32, (rows, length), 0)
        c = lax.broadcasted_iota(jnp.int32, (rows, length), 1)
        return jnp.where(c == (r & (SUB - 1)) * run + (r >> 3) + base, 1.0, 0.0).astype(bf16)

    order = picks(length, 0)
    extended[pl.ds(lead, length), :] = dot(order, inner[...])
    extended[pl.ds(0, lead), :] = dot(picks(lead, 1 - taps), inner[...])

    smooth = extended[pl.ds(0, length), :] * conv[0:1, :]
    for tap in range(1, taps):
        smooth = smooth + extended[pl.ds(tap * SUB, length), :] * conv[tap : tap + 1, :]
    smoothed[...] = smooth.astype(bf16)

    heads, block = w_decay.shape[0], w_decay.shape[1]
    wide = blocks.shape[1]
    per = wide // block
    blocks[...] = jnp.zeros_like(blocks)
    for head in range(heads):
        q, i = head // per, (head % per) * block
        blocks[q, pl.ds(i, block), pl.ds(i, block)] = -w_decay[head]
        blocks[q, pl.ds(i, block), pl.ds(wide + i, block)] = -w_input[head]

    def store(at, r, i):
        pre_r[:, at] = r
        pre_i[:, at] = i

    block_dots(smoothed, blocks, store)

    part0 = offset[...].astype(bf16).astype(f32)
    part1 = (offset[...] - part0).astype(bf16).astype(f32)
    part2 = offset[...] - part0 - part1
    parts = jnp.concatenate([part0, part1, part2, jnp.zeros_like(part0)], axis=0).astype(bf16)
    moved = lax.dot_general(parts, order, (((1,), (1,)), ((), ())), preferred_element_type=f32).astype(bf16)
    r = lax.broadcasted_iota(jnp.int32, (4 * heads, width), 0)
    c = lax.broadcasted_iota(jnp.int32, (4 * heads, width), 1)
    spread = jnp.where((r & (heads - 1)) == (c >> 6), 1.0, 0.0).astype(bf16)
    shift[...] = lax.dot_general(moved, spread, (((0,), (0,)), ((), ())), preferred_element_type=f32)
    heads_shift[...] = shift[pl.ds(0, heads_shift.shape[0]), :]

    rows = 4 * SUB

    def scan_rows(i, carry, skip=0):
        h, p = carry
        at = pl.ds(pl.multiple_of(i * rows, rows), rows)
        decay, drive = gates(
            pre_r[at, :], pre_i[at, :], smoothed[at, :].astype(f32), b_decay[...], b_input[...], rate[...], shift[at, :]
        )
        known = lax.broadcasted_iota(jnp.int32, (SUB, width), 0) > 0
        for k in range(rows // SUB):
            a, b = decay[k * SUB : (k + 1) * SUB, :], drive[k * SUB : (k + 1) * SUB, :]
            if k < skip:
                a, b = jnp.where(known, a, 1.0), jnp.where(known, b, 0.0)
            h = a * h + b
            p = a * p
            here = pl.ds(pl.multiple_of(i * rows + k * SUB, SUB), SUB)
            h_out[here, :] = h
            p_out[here, :] = p
        return h, p

    start = (jnp.zeros((SUB, width), f32), jnp.ones((SUB, width), f32))
    h, p = start
    half, blocks_half = length // 2, length // rows // 2
    tp = lax.axis_index("tp")
    for c, (normed, place) in enumerate(((normed_own, tp), (normed_other, 1 - tp))):
        at = pl.ds(pl.multiple_of(place * half, half), half)
        gate[at, :] = dot(normed[...], w_gate[...]).astype(bf16)
        for i in range(c * blocks_half, (c + 1) * blocks_half):
            h, p = scan_rows(i, (h, p), 0 if i else taps - 1)
    each = length // 4
    for c in range(0, length, each):
        g_out[c : c + each, :] = jax.nn.gelu(dot(order[c : c + each], gate[...]))
    ends_out[0] = p
    ends_out[1] = h


def head_kernel(
    inner, halo, conv, blocks, b_decay, b_input, rate, shift, ends,
    runs_out, heads_out, sent_out,
    near, smoothed, pre_r, pre_i,
):
    width = inner.shape[1]
    taps = conv.shape[0]
    near[pl.ds(0, HALO), :] = halo[...].astype(f32)
    near[pl.ds(HALO, HALO), :] = inner[pl.ds(0, 2 * HALO), :].astype(f32)[:HALO]
    smooth = near[pl.ds(HALO - taps + 1, HALO), :] * conv[0:1, :]
    for tap in range(1, taps):
        smooth = smooth + near[pl.ds(HALO - taps + 1 + tap, HALO), :] * conv[tap : tap + 1, :]
    smoothed[...] = jnp.concatenate([smooth, jnp.zeros_like(smooth)], axis=0).astype(bf16)

    def store(at, r, i):
        pre_r[:, at] = r[:HALO]
        pre_i[:, at] = i[:HALO]

    block_dots(smoothed, blocks, store)
    shifts = jnp.concatenate([shift[pl.ds(k * SUB, 1), :] for k in range(HALO)], axis=0)
    decay, drive = gates(
        pre_r[...], pre_i[...], smoothed[...].astype(f32)[:HALO], b_decay[...], b_input[...], rate[...], shifts
    )
    a_before, b_before = jnp.ones((1, width), f32), jnp.zeros((1, width), f32)
    for k in range(taps - 1):
        a_k = decay[k : k + 1, :]
        a_before, b_before = a_before * a_k, a_k * b_before + drive[k : k + 1, :]
        heads_out[0, k : k + 1, :] = a_before
        heads_out[1, k : k + 1, :] = b_before
    for s in range(SUB):
        runs_out[0, s : s + 1, :] = a_before
        runs_out[1, s : s + 1, :] = b_before
        a_s = ends[0, s : s + 1, :]
        a_before, b_before = a_before * a_s, a_s * b_before + ends[1, s : s + 1, :]
    pair = jnp.concatenate([a_before, b_before], axis=0)
    sent_out[...] = jnp.broadcast_to(pair[None], sent_out.shape)


def before_in(pieces, index):
    width = pieces.shape[2]
    a, b = jnp.ones((1, width), f32), jnp.zeros((1, width), f32)
    a_at, b_at = a, b
    for k in range(pieces.shape[0]):
        here = k == index
        a_at, b_at = jnp.where(here, a, a_at), jnp.where(here, b, b_at)
        a_k, b_k = pieces[k, 0:1, :], pieces[k, 1:2, :]
        a, b = a * a_k, a_k * b + b_k
    return (a_at, b_at), (a, b)


def plane_kernel(pieces, before_out, sent_out):
    index = lax.axis_index("sp_1") * lax.axis_size("sp_2") + lax.axis_index("sp_2")
    (a_at, b_at), (a, b) = before_in(pieces, index)
    before_out[...] = jnp.concatenate([a_at, b_at], axis=0)
    pair = jnp.concatenate([a, b], axis=0)
    sent_out[...] = jnp.broadcast_to(pair[None], sent_out.shape)


def back(gated, first):
    length = gated.shape[0]
    half, run = length // 2, length // SUB
    t = lax.broadcasted_iota(jnp.int32, (half, length), 0) + first
    c = lax.broadcasted_iota(jnp.int32, (half, length), 1)
    pick = jnp.where(t == (c & (SUB - 1)) * run + (c >> 3), 1.0, 0.0).astype(bf16)
    return dot(pick, gated[...]).astype(bf16)


def state_kernel(pieces, before, runs, heads, h, p, g, w_mine, gated, theirs_out):
    (_, b_at), _ = before_in(pieces, lax.axis_index("sp_0"))
    carried = before[0:1, :] * b_at + before[1:2, :]
    start = runs[0] * carried + runs[1]
    length = h.shape[0]
    rows = 4 * SUB
    opening = heads[0] * carried + heads[1]
    first = [jnp.concatenate([opening[k : k + 1], start[1:]], axis=0) for k in range(heads.shape[1])]
    groups = rows // SUB

    def state_rows(i, starts):
        at = pl.ds(pl.multiple_of(i * rows, rows), rows)
        gated[at, :] = ((h[at, :] + p[at, :] * starts) * g[at, :]).astype(bf16)
        return starts

    state_rows(0, jnp.concatenate(first + [start] * (groups - len(first)), axis=0))
    starts = jnp.concatenate([start] * groups, axis=0)
    lax.fori_loop(1, length // rows, lambda i, _: (state_rows(i, starts), 0)[1], 0)
    theirs = back(gated, (1 - lax.axis_index("tp")) * (length // 2))
    theirs_out[...] = dot(theirs, w_mine[...]).astype(bf16)


def own_kernel(gated, w_mine, part):
    mine = back(gated, lax.axis_index("tp") * (gated.shape[0] // 2))
    part[...] = dot(mine, w_mine[...])


def out_kernel(part, received, out, block, sent):
    rows = block.shape[1]
    copies = []
    for i in range(block.shape[0]):
        at = pl.ds(i * rows, rows)
        block[i] = (part[at, :] + received[at, :].astype(f32)).astype(bf16)
        copies.append(pltpu.make_async_copy(block.at[i], out.at[at, :], sent.at[i]))
        copies[i].start()
    for copy in copies:
        copy.wait()


VMEM = pl.BlockSpec(memory_space=pltpu.VMEM)


HBM = pl.BlockSpec(memory_space=pltpu.HBM)
LATER = 8


def call(kernel, inputs, out_shape, scratch=(), out_specs=None):
    run = pl.pallas_call(
        kernel,
        out_shape=out_shape,
        out_specs=out_specs or jax.tree.map(lambda _: VMEM, out_shape),
        scratch_shapes=list(scratch),
        compiler_params=pltpu.CompilerParams(vmem_limit_bytes=32 * 1024 * 1024),
        in_specs=[VMEM] * inputs[0] + [HBM] * inputs[1],
    )

    def place(i, a):
        return pltpu.with_memory_space_constraint(a, pltpu.VMEM if i < inputs[0] else pltpu.HBM)

    return lambda *args: run(*(place(i, a) for i, a in enumerate(args)))


def step(
    tokens,
    norm_gain,
    in_weight,
    gate_weight,
    conv_weight,
    decay_gate_weight,
    decay_gate_bias,
    input_gate_weight,
    input_gate_bias,
    channel_decay_rate,
    forgetting_offset,
    out_weight,
):
    half, features = tokens.shape
    length = 2 * half
    width = in_weight.shape[1]
    heads, block = decay_gate_weight.shape[:2]
    count = lax.axis_size(SP)
    plane = lax.axis_size(PLANE)
    deep = lax.axis_size("sp_0")
    S = jax.ShapeDtypeStruct

    swap = [(0, 1), (1, 0)]
    other = lax.ppermute(tokens, "tp", swap)

    row = lambda v: v.reshape(1, -1)
    later = (
        gate_weight, conv_weight, decay_gate_weight, row(decay_gate_bias),
        input_gate_weight, row(input_gate_bias), row(channel_decay_rate), forgetting_offset,
    )
    big = pltpu.VMEM
    like = lambda a: big(a.shape, a.dtype)
    square = big((length, width), f32)
    stats = [big((half, 128), f32), big((half, 128), f32)]
    gain = row(norm_gain)
    inner_own, normed_own, gain, w_in = call(
        own_tokens_kernel,
        (0, 3),
        (big((half, width), bf16), big((half, features), bf16), like(gain), like(in_weight)),
        scratch=[like(tokens), pltpu.SemaphoreType.DMA((3,)), *stats],
    )(gain, in_weight, tokens)
    inner, tail, normed_other, *held = call(
        other_tokens_kernel,
        (4, LATER),
        (
            big((length, width), bf16), big((HALO, width), bf16), big((half, features), bf16),
            *(like(a) for a in later),
        ),
        scratch=[pltpu.SemaphoreType.DMA((LATER,)), *stats],
    )(other, gain, w_in, inner_own, *later)
    w_gate, conv, w_decay, b_decay, w_input, b_input, rate, offset = held
    halo = lax.ppermute(tail, SP, [(s, s + 1) for s in range(count - 1)])
    taps = conv_weight.shape[0]
    h, p, g, ends, blocks, shift = call(
        scan_kernel,
        (11, 0),
        (
            square, square, square, big((2, SUB, width), f32),
            big((heads * block // 256, 256, 512), bf16), big((HALO * SUB, width), f32),
        ),
        scratch=[
            big((length, width), bf16), square, square, square,
            big((length + (taps - 1) * SUB, width), f32), big((length, width), bf16),
        ],
    )(inner, normed_own, normed_other, w_gate, conv, w_decay, b_decay, w_input, b_input, rate, offset)
    runs, opening, sent = call(
        head_kernel,
        (9, 0),
        (big((2, SUB, width), f32), big((2, taps - 1, width), f32), big((plane, 2, width), f32)),
        scratch=[
            big((2 * HALO, width), f32), big((2 * HALO, width), bf16),
            big((HALO, width), f32), big((HALO, width), f32),
        ],
    )(inner, halo, conv, blocks, b_decay, b_input, rate, shift, ends)
    pieces = lax.all_to_all(sent, PLANE, split_axis=0, concat_axis=0, tiled=True)
    before, sent = call(plane_kernel, (1, 0), (big((2, width), f32), big((deep, 2, width), f32)))(pieces)
    pieces = lax.all_to_all(sent, "sp_0", split_axis=0, concat_axis=0, tiled=True)
    gated, theirs = call(
        state_kernel, (8, 0), (big((length, width), bf16), big((half, features), bf16))
    )(pieces, before, runs, opening, h, p, g, out_weight)
    received = lax.ppermute(theirs, "tp", swap)
    part = call(own_kernel, (2, 0), big((half, features), f32))(gated, out_weight)
    rows = 64
    return call(
        out_kernel,
        (2, 0),
        S((half, features), bf16),
        scratch=(big((half // rows, rows, features), bf16), pltpu.SemaphoreType.DMA((half // rows,))),
        out_specs=HBM,
    )(part, received)


def solution(mesh):
    torus = Mesh(mesh.devices.reshape(8, 8, 4, mesh.shape["tp"]), SP_TP)
    placed = (
        P(SP_TP, None),
        P(),
        P(None, "tp"),
        P(None, "tp"),
        P(None, "tp"),
        P("tp", None, None),
        P("tp"),
        P("tp", None, None),
        P("tp"),
        P("tp"),
        P("tp", SP),
        P("tp", None),
    )
    return jax.shard_map(step, mesh=torus, in_specs=placed, out_specs=P(SP_TP, None), check_vma=False)
```

```python
import jax
import jax.numpy as jnp
from jax import lax
from jax.experimental import pallas as pl
from jax.experimental.pallas import tpu as pltpu
from jax.sharding import Mesh
from jax.sharding import PartitionSpec as P

SP = ("sp_0", "sp_1", "sp_2")
PLANE = ("sp_1", "sp_2")
SP_TP = ("sp_0", "sp_1", "sp_2", "tp")

EPSILON = 1e-05
SUB = 8
HALO = 8
f32, bf16 = jnp.float32, jnp.bfloat16


def dot(a, b):
    return jnp.dot(a, b, preferred_element_type=f32)


def norm_tokens(source, target, gain, middle, scale, ready=None):
    half, features = source.shape
    step, lanes = 32, 128

    def tiles(r):
        return [source[r, t : t + lanes].astype(f32) for t in range(0, features, lanes)]

    def by_rows(one):
        def rows(i, _):
            one(pl.ds(pl.multiple_of(i * step, step), step))
            return 0

        lax.fori_loop(0, half // step, rows, 0)

    def over_features(stat):
        return jnp.broadcast_to(jnp.sum(stat[...], axis=1, keepdims=True) * (1.0 / features), stat.shape)

    def add_up(r):
        middle[r, :] = sum(tiles(r))

    by_rows(add_up)
    middle[...] = over_features(middle)

    def add_squares(r):
        m = middle[r, :]
        scale[r, :] = sum((x - m) * (x - m) for x in tiles(r))

    by_rows(add_squares)
    scale[...] = lax.rsqrt(over_features(scale) + EPSILON)
    if ready is not None:
        ready.wait()

    def write(r):
        m, k = middle[r, :], scale[r, :]
        for t, x in zip(range(0, features, lanes), tiles(r)):
            target[r, t : t + lanes] = ((x - m) * k * gain[:, t : t + lanes]).astype(bf16)

    by_rows(write)


def fetch(stored, held, arrived, order):
    copies = [pltpu.make_async_copy(a, b, arrived.at[i]) for i, (a, b) in enumerate(zip(stored, held))]
    for i in order:
        copies[i].start()
    return copies


def own_tokens_kernel(gain_in, w_in_in, own_in, inner, normed, gain, w_in, own, arrived, middle, scale):
    copies = fetch((gain_in, w_in_in, own_in), (gain, w_in, own), arrived, (2, 0, 1))
    copies[2].wait()
    norm_tokens(own, normed, gain, middle, scale, copies[0])
    copies[1].wait()
    inner[...] = dot(normed[...], w_in[...]).astype(bf16)


def other_tokens_kernel(other, gain, w_in, inner_own, *refs):
    stored, refs = refs[:LATER], refs[LATER:]
    inner, tail, normed, *held = refs[: 3 + LATER]
    arrived, middle, scale = refs[3 + LATER :]
    copies = fetch(stored, held, arrived, range(LATER))
    half = other.shape[0]
    tp = lax.axis_index("tp")
    norm_tokens(other, normed, gain, middle, scale)
    inner[pl.ds(pl.multiple_of(tp * half, half), half), :] = inner_own[...]
    there = pl.ds(pl.multiple_of((1 - tp) * half, half), half)
    inner[there, :] = dot(normed[...], w_in[...]).astype(bf16)
    tail[...] = inner[pl.ds(2 * half - 2 * HALO, 2 * HALO), :].astype(f32)[HALO:].astype(bf16)
    for copy in copies:
        copy.wait()


def gates(minus_r, minus_i, x, b_decay, b_input, rate, shift):
    retain = 1.0 / (1.0 + jnp.exp(minus_r - b_decay))
    admit = 1.0 / (1.0 + jnp.exp(minus_i - b_input))
    log_decay = retain * (-8.0 * rate) + shift
    decay = jnp.exp(log_decay)
    rest = jnp.tanh(log_decay) * (-1.0 - decay * decay)
    return decay, rest * lax.rsqrt(jnp.maximum(rest, 1e-37)) * admit * x


def block_dots(smoothed, blocks, store):
    wide = blocks.shape[1]
    for q in range(blocks.shape[0]):
        at = slice(q * wide, (q + 1) * wide)
        both = dot(smoothed[:, at], blocks[q])
        store(at, both[:, :wide], both[:, wide:])


def scan_kernel(
    inner, normed_own, normed_other, w_gate, conv, w_decay, b_decay, w_input, b_input, rate, offset,
    h_out, p_out, g_out, ends_out, blocks, heads_shift,
    smoothed, pre_r, pre_i, shift, extended, gate,
):
    length, width = inner.shape
    run = length // SUB
    taps = conv.shape[0]
    lead = (taps - 1) * SUB

    def picks(rows, base):
        r = lax.broadcasted_iota(jnp.int32, (rows, length), 0)
        c = lax.broadcasted_iota(jnp.int32, (rows, length), 1)
        return jnp.where(c == (r & (SUB - 1)) * run + (r >> 3) + base, 1.0, 0.0).astype(bf16)

    order = picks(length, 0)
    extended[pl.ds(lead, length), :] = dot(order, inner[...])
    extended[pl.ds(0, lead), :] = dot(picks(lead, 1 - taps), inner[...])

    smooth = extended[pl.ds(0, length), :] * conv[0:1, :]
    for tap in range(1, taps):
        smooth = smooth + extended[pl.ds(tap * SUB, length), :] * conv[tap : tap + 1, :]
    smoothed[...] = smooth.astype(bf16)

    heads, block = w_decay.shape[0], w_decay.shape[1]
    wide = blocks.shape[1]
    per = wide // block
    blocks[...] = jnp.zeros_like(blocks)
    for head in range(heads):
        q, i = head // per, (head % per) * block
        blocks[q, pl.ds(i, block), pl.ds(i, block)] = -w_decay[head]
        blocks[q, pl.ds(i, block), pl.ds(wide + i, block)] = -w_input[head]

    def store(at, r, i):
        pre_r[:, at] = r
        pre_i[:, at] = i

    block_dots(smoothed, blocks, store)

    part0 = offset[...].astype(bf16).astype(f32)
    part1 = (offset[...] - part0).astype(bf16).astype(f32)
    part2 = offset[...] - part0 - part1
    parts = jnp.concatenate([part0, part1, part2, jnp.zeros_like(part0)], axis=0).astype(bf16)
    moved = lax.dot_general(parts, order, (((1,), (1,)), ((), ())), preferred_element_type=f32).astype(bf16)
    r = lax.broadcasted_iota(jnp.int32, (4 * heads, width), 0)
    c = lax.broadcasted_iota(jnp.int32, (4 * heads, width), 1)
    spread = jnp.where((r & (heads - 1)) == (c >> 6), 1.0, 0.0).astype(bf16)
    shift[...] = lax.dot_general(moved, spread, (((0,), (0,)), ((), ())), preferred_element_type=f32)
    heads_shift[...] = shift[pl.ds(0, heads_shift.shape[0]), :]

    rows = 4 * SUB

    def scan_rows(i, carry, skip=0):
        h, p = carry
        at = pl.ds(pl.multiple_of(i * rows, rows), rows)
        decay, drive = gates(
            pre_r[at, :], pre_i[at, :], smoothed[at, :].astype(f32), b_decay[...], b_input[...], rate[...], shift[at, :]
        )
        known = lax.broadcasted_iota(jnp.int32, (SUB, width), 0) > 0
        for k in range(rows // SUB):
            a, b = decay[k * SUB : (k + 1) * SUB, :], drive[k * SUB : (k + 1) * SUB, :]
            if k < skip:
                a, b = jnp.where(known, a, 1.0), jnp.where(known, b, 0.0)
            h = a * h + b
            p = a * p
            here = pl.ds(pl.multiple_of(i * rows + k * SUB, SUB), SUB)
            h_out[here, :] = h
            p_out[here, :] = p
        return h, p

    start = (jnp.zeros((SUB, width), f32), jnp.ones((SUB, width), f32))
    h, p = start
    half, blocks_half = length // 2, length // rows // 2
    tp = lax.axis_index("tp")
    for c, (normed, place) in enumerate(((normed_own, tp), (normed_other, 1 - tp))):
        at = pl.ds(pl.multiple_of(place * half, half), half)
        gate[at, :] = dot(normed[...], w_gate[...]).astype(bf16)
        for i in range(c * blocks_half, (c + 1) * blocks_half):
            h, p = scan_rows(i, (h, p), 0 if i else taps - 1)
    each = length // 4
    for c in range(0, length, each):
        g_out[c : c + each, :] = jax.nn.gelu(dot(order[c : c + each], gate[...]))
    ends_out[0] = p
    ends_out[1] = h


def pack_kernel(
    inner, halo, conv, blocks, b_decay, b_input, rate, shift, ends, h, p, g, weight,
    runs_out, mine_out, packed_out, sent_out,
    near, smoothed, pre_r, pre_i, gated_h, gated_p, arrived,
):
    length, width = inner.shape
    half, run = length // 2, length // SUB
    taps = conv.shape[0]
    cols = weight.shape[1] // width
    copies = [
        pltpu.make_async_copy(
            weight.at[:, pl.ds(q * width, width)], packed_out.at[pl.ds((q + 1) * width, width)], arrived.at[q]
        )
        for q in range(cols)
    ]
    for copy in copies:
        copy.start()
    near[pl.ds(0, HALO), :] = halo[...].astype(f32)
    near[pl.ds(HALO, HALO), :] = inner[pl.ds(0, 2 * HALO), :].astype(f32)[:HALO]
    smooth = near[pl.ds(HALO - taps + 1, HALO), :] * conv[0:1, :]
    for tap in range(1, taps):
        smooth = smooth + near[pl.ds(HALO - taps + 1 + tap, HALO), :] * conv[tap : tap + 1, :]
    smoothed[...] = jnp.concatenate([smooth, jnp.zeros_like(smooth)], axis=0).astype(bf16)

    def store(at, r, i):
        pre_r[:, at] = r[:HALO]
        pre_i[:, at] = i[:HALO]

    block_dots(smoothed, blocks, store)
    shifts = jnp.concatenate([shift[pl.ds(k * SUB, 1), :] for k in range(HALO)], axis=0)
    decay, drive = gates(
        pre_r[...], pre_i[...], smoothed[...].astype(f32)[:HALO], b_decay[...], b_input[...], rate[...], shifts
    )
    one, zero = jnp.ones((1, width), f32), jnp.zeros((1, width), f32)
    a_head, b_head, opening = one, zero, []
    for k in range(taps - 1):
        a_k = decay[k : k + 1, :]
        a_head, b_head = a_head * a_k, a_k * b_head + drive[k : k + 1, :]
        opening.append((a_head, b_head))
    runs_a, runs_b = [one], [zero]
    a_before, b_before = a_head, b_head
    for s in range(SUB):
        a_s = ends[0, s : s + 1, :]
        a_before, b_before = a_before * a_s, a_s * b_before + ends[1, s : s + 1, :]
        runs_a.append(a_before)
        runs_b.append(b_before)
    pair = jnp.concatenate([a_before, b_before], axis=0)
    sent_out[...] = jnp.broadcast_to(pair[None], sent_out.shape)
    runs = jnp.concatenate(runs_a[:SUB] + runs_b[:SUB], axis=0)
    runs_out[...] = runs

    first = lax.broadcasted_iota(jnp.int32, (SUB, width), 0) == 0
    times = jnp.where(first, a_head, 1.0)
    plus = jnp.where(first, b_head, 0.0)
    rows = 4 * SUB
    times, plus = (jnp.concatenate([v] * (rows // SUB), axis=0) for v in (times, plus))

    def gate_rows(i, patch=False):
        at = pl.ds(pl.multiple_of(i * rows, rows), rows)
        ph, pp, pg = h[at, :], p[at, :], g[at, :]
        ph, pp = ph + pp * plus, pp * times
        if patch:
            r = lax.broadcasted_iota(jnp.int32, (rows, width), 0)
            for k, (a_k, b_k) in enumerate(opening):
                ph, pp = jnp.where(r == k * SUB, b_k, ph), jnp.where(r == k * SUB, a_k, pp)
        gated_h[at, :] = (ph * pg).astype(bf16)
        gated_p[at, :] = (pp * pg).astype(bf16)

    gate_rows(0, True)
    lax.fori_loop(1, length // rows, lambda i, _: (gate_rows(i), 0)[1], 0)

    def back(gated, begin):
        t = lax.broadcasted_iota(jnp.int32, (half, length), 0) + begin
        c = lax.broadcasted_iota(jnp.int32, (half, length), 1)
        pick = jnp.where(t == (c & (SUB - 1)) * run + (c >> 3), 1.0, 0.0).astype(bf16)
        return dot(pick, gated[...]).astype(bf16)

    tp = lax.axis_index("tp")
    for i, gated in enumerate((gated_h, gated_p)):
        packed_out[pl.ds(i * half, half), :] = back(gated, (1 - tp) * half)
        mine_out[pl.ds(i * half, half), :] = back(gated, tp * half)
    rest = runs
    for i in range(PARTS):
        part = rest.astype(bf16)
        packed_out[pl.ds((cols + 1) * width + i * 2 * SUB, 2 * SUB), :] = part
        rest = rest - part.astype(f32)
    for copy in copies:
        copy.wait()


def before_in(pieces, index):
    width = pieces[0].shape[1]
    a, b = jnp.ones((1, width), f32), jnp.zeros((1, width), f32)
    a_at, b_at = a, b
    for k, piece in enumerate(pieces):
        here = k == index
        a_at, b_at = jnp.where(here, a, a_at), jnp.where(here, b, b_at)
        a_k, b_k = piece[0:1], piece[1:2]
        a, b = a * a_k, a_k * b + b_k
    return (a_at, b_at), (a, b)


def plane_kernel(pieces, before_out, sent_out):
    index = lax.axis_index("sp_1") * lax.axis_size("sp_2") + lax.axis_index("sp_2")
    (a_at, b_at), (a, b) = before_in([pieces[k] for k in range(pieces.shape[0])], index)
    before = jnp.concatenate([a_at, b_at], axis=0)
    before_out[...] = before
    pair = jnp.concatenate([a, b], axis=0)
    partner = lax.axis_index("sp_0") * 2 + 1 - lax.axis_index("tp")
    for k in range(sent_out.shape[0]):
        sent_out[k] = jnp.where(k == partner, before, pair)


def out_kernel(pieces, before, runs, mine, packed, received, out, theirs, block, gated_mine, gated_theirs, sent):
    half, width = out.shape[0], mine.shape[1]
    run = half // (SUB // 2)
    deep = pieces.shape[0] // 2
    at, tp = lax.axis_index("sp_0"), lax.axis_index("tp")
    is_one = tp == 1
    for k in range(deep):
        theirs[k] = jnp.where(is_one, pieces[2 * k], pieces[2 * k + 1])
    own = [jnp.where(is_one, pieces[2 * k + 1], pieces[2 * k]) for k in range(deep)]
    cols = out.shape[1] // width
    last = (cols + 1) * width
    their_runs = sum(received[pl.ds(last + i * 2 * SUB, 2 * SUB), :].astype(f32) for i in range(PARTS))
    sides = (
        (own, before[...], runs[...], mine, gated_mine),
        ([theirs[k] for k in range(deep)], theirs[at], their_runs, received, gated_theirs),
    )
    for totals, near, steps, parts, gated in sides:
        (_, b_at), _ = before_in(totals, at)
        carried = near[0:1] * b_at + near[1:2]
        start = steps[:SUB] * carried + steps[SUB:]
        start = jnp.where(is_one, start[SUB // 2 :], start[: SUB // 2])
        for u in range(SUB // 2):
            here, there = pl.ds(u * run, run), pl.ds(half + u * run, run)
            gated[here, :] = (
                parts[here, :].astype(f32) + parts[there, :].astype(f32) * start[u : u + 1]
            ).astype(bf16)
    copies = []
    for q in range(cols):
        w = pl.ds((q + 1) * width, width)
        block[q] = (dot(gated_mine[...], packed[w, :]) + dot(gated_theirs[...], received[w, :])).astype(bf16)
        copies.append(pltpu.make_async_copy(block.at[q], out.at[:, pl.ds(q * width, width)], sent.at[q]))
        copies[q].start()
    for copy in copies:
        copy.wait()


VMEM = pl.BlockSpec(memory_space=pltpu.VMEM)


HBM = pl.BlockSpec(memory_space=pltpu.HBM)
PARTS = 3
LATER = 8


def call(kernel, inputs, out_shape, scratch=(), out_specs=None):
    run = pl.pallas_call(
        kernel,
        out_shape=out_shape,
        out_specs=out_specs or jax.tree.map(lambda _: VMEM, out_shape),
        scratch_shapes=list(scratch),
        compiler_params=pltpu.CompilerParams(vmem_limit_bytes=32 * 1024 * 1024),
        in_specs=[VMEM] * inputs[0] + [HBM] * inputs[1],
    )

    def place(i, a):
        return pltpu.with_memory_space_constraint(a, pltpu.VMEM if i < inputs[0] else pltpu.HBM)

    return lambda *args: run(*(place(i, a) for i, a in enumerate(args)))


def step(
    tokens,
    norm_gain,
    in_weight,
    gate_weight,
    conv_weight,
    decay_gate_weight,
    decay_gate_bias,
    input_gate_weight,
    input_gate_bias,
    channel_decay_rate,
    forgetting_offset,
    out_weight,
):
    half, features = tokens.shape
    length = 2 * half
    width = in_weight.shape[1]
    heads, block = decay_gate_weight.shape[:2]
    count = lax.axis_size(SP)
    plane = lax.axis_size(PLANE)
    deep = lax.axis_size("sp_0")
    S = jax.ShapeDtypeStruct

    swap = [(0, 1), (1, 0)]
    other = lax.ppermute(tokens, "tp", swap)

    row = lambda v: v.reshape(1, -1)
    later = (
        gate_weight, conv_weight, decay_gate_weight, row(decay_gate_bias),
        input_gate_weight, row(input_gate_bias), row(channel_decay_rate), forgetting_offset,
    )
    big = pltpu.VMEM
    like = lambda a: big(a.shape, a.dtype)
    square = big((length, width), f32)
    stats = [big((half, 128), f32), big((half, 128), f32)]
    gain = row(norm_gain)
    inner_own, normed_own, gain, w_in = call(
        own_tokens_kernel,
        (0, 3),
        (big((half, width), bf16), big((half, features), bf16), like(gain), like(in_weight)),
        scratch=[like(tokens), pltpu.SemaphoreType.DMA((3,)), *stats],
    )(gain, in_weight, tokens)
    inner, tail, normed_other, *held = call(
        other_tokens_kernel,
        (4, LATER),
        (
            big((length, width), bf16), big((HALO, width), bf16), big((half, features), bf16),
            *(like(a) for a in later),
        ),
        scratch=[pltpu.SemaphoreType.DMA((LATER,)), *stats],
    )(other, gain, w_in, inner_own, *later)
    w_gate, conv, w_decay, b_decay, w_input, b_input, rate, offset = held
    halo = lax.ppermute(tail, SP, [(s, s + 1) for s in range(count - 1)])
    taps = conv_weight.shape[0]
    h, p, g, ends, blocks, shift = call(
        scan_kernel,
        (11, 0),
        (
            square, square, square, big((2, SUB, width), f32),
            big((heads * block // 256, 256, 512), bf16), big((HALO * SUB, width), f32),
        ),
        scratch=[
            big((length, width), bf16), square, square, square,
            big((length + (taps - 1) * SUB, width), f32), big((length, width), bf16),
        ],
    )(inner, normed_own, normed_other, w_gate, conv, w_decay, b_decay, w_input, b_input, rate, offset)
    cols = features // width
    packed_rows = (cols + 1) * width + PARTS * 2 * SUB
    runs, mine, packed, sent = call(
        pack_kernel,
        (12, 1),
        (
            big((2 * SUB, width), f32), big((length, width), bf16),
            big((packed_rows, width), bf16), big((plane, 2, width), f32),
        ),
        scratch=[
            big((2 * HALO, width), f32), big((2 * HALO, width), bf16),
            big((HALO, width), f32), big((HALO, width), f32),
            big((length, width), bf16), big((length, width), bf16),
            pltpu.SemaphoreType.DMA((cols,)),
        ],
    )(inner, halo, conv, blocks, b_decay, b_input, rate, shift, ends, h, p, g, out_weight)
    received = lax.ppermute(packed, "tp", swap)
    pieces = lax.all_to_all(sent, PLANE, split_axis=0, concat_axis=0, tiled=True)
    before, sent = call(plane_kernel, (1, 0), (big((2, width), f32), big((2 * deep, 2, width), f32)))(pieces)
    pieces = lax.all_to_all(sent, ("sp_0", "tp"), split_axis=0, concat_axis=0, tiled=True)
    return call(
        out_kernel,
        (6, 0),
        S((half, features), bf16),
        scratch=(
            big((deep, 2, width), f32), big((cols, half, width), bf16),
            big((half, width), bf16), big((half, width), bf16), pltpu.SemaphoreType.DMA((cols,)),
        ),
        out_specs=HBM,
    )(pieces, before, runs, mine, packed, received)


def solution(mesh):
    torus = Mesh(mesh.devices.reshape(8, 8, 4, mesh.shape["tp"]), SP_TP)
    placed = (
        P(SP_TP, None),
        P(),
        P(None, "tp"),
        P(None, "tp"),
        P(None, "tp"),
        P("tp", None, None),
        P("tp"),
        P("tp", None, None),
        P("tp"),
        P("tp"),
        P("tp", SP),
        P("tp", None),
    )
    return jax.shard_map(step, mesh=torus, in_specs=placed, out_specs=P(SP_TP, None), check_vma=False)
```

```python
import jax
import jax.numpy as jnp
from jax import lax
from jax.experimental import pallas as pl
from jax.experimental.pallas import tpu as pltpu
from jax.sharding import Mesh
from jax.sharding import PartitionSpec as P

SP = ("sp_0", "sp_1", "sp_2")
PLANE = ("sp_1", "sp_2")
SP_TP = ("sp_0", "sp_1", "sp_2", "tp")

EPSILON = 1e-05
SUB = 8
HALO = 8
f32, bf16 = jnp.float32, jnp.bfloat16


def dot(a, b):
    return jnp.dot(a, b, preferred_element_type=f32)


def norm_tokens(source, target, gain, middle, scale, ready=None):
    half, features = source.shape
    step, lanes = 32, 128

    def tiles(r):
        return [source[r, t : t + lanes].astype(f32) for t in range(0, features, lanes)]

    def by_rows(one):
        def rows(i, _):
            one(pl.ds(pl.multiple_of(i * step, step), step))
            return 0

        lax.fori_loop(0, half // step, rows, 0)

    def over_features(stat):
        return jnp.broadcast_to(jnp.sum(stat[...], axis=1, keepdims=True) * (1.0 / features), stat.shape)

    def add_up(r):
        middle[r, :] = sum(tiles(r))

    by_rows(add_up)
    middle[...] = over_features(middle)

    def add_squares(r):
        m = middle[r, :]
        scale[r, :] = sum((x - m) * (x - m) for x in tiles(r))

    by_rows(add_squares)
    scale[...] = lax.rsqrt(over_features(scale) + EPSILON)
    if ready is not None:
        ready.wait()

    def write(r):
        m, k = middle[r, :], scale[r, :]
        for t, x in zip(range(0, features, lanes), tiles(r)):
            target[r, t : t + lanes] = ((x - m) * k * gain[:, t : t + lanes]).astype(bf16)

    by_rows(write)


def fetch(stored, held, arrived, order):
    copies = [pltpu.make_async_copy(a, b, arrived.at[i]) for i, (a, b) in enumerate(zip(stored, held))]
    for i in order:
        copies[i].start()
    return copies


def own_tokens_kernel(gain_in, w_in_in, own_in, inner, normed, gain, w_in, own, arrived, middle, scale):
    copies = fetch((gain_in, w_in_in, own_in), (gain, w_in, own), arrived, (2, 0, 1))
    copies[2].wait()
    norm_tokens(own, normed, gain, middle, scale, copies[0])
    copies[1].wait()
    inner[...] = dot(normed[...], w_in[...]).astype(bf16)


def other_tokens_kernel(other, gain, w_in, inner_own, *refs):
    stored, refs = refs[:LATER], refs[LATER:]
    inner, tail, normed, *held = refs[: 3 + LATER]
    arrived, middle, scale = refs[3 + LATER :]
    copies = fetch(stored, held, arrived, range(LATER))
    half = other.shape[0]
    tp = lax.axis_index("tp")
    norm_tokens(other, normed, gain, middle, scale)
    inner[pl.ds(pl.multiple_of(tp * half, half), half), :] = inner_own[...]
    there = pl.ds(pl.multiple_of((1 - tp) * half, half), half)
    inner[there, :] = dot(normed[...], w_in[...]).astype(bf16)
    tail[...] = inner[pl.ds(2 * half - 2 * HALO, 2 * HALO), :].astype(f32)[HALO:].astype(bf16)
    for copy in copies:
        copy.wait()


def gates(minus_r, minus_i, x, b_decay, b_input, rate, shift):
    retain = 1.0 / (1.0 + jnp.exp(minus_r - b_decay))
    admit = 1.0 / (1.0 + jnp.exp(minus_i - b_input))
    log_decay = retain * (-8.0 * rate) + shift
    decay = jnp.exp(log_decay)
    rest = jnp.tanh(log_decay) * (-1.0 - decay * decay)
    return decay, rest * lax.rsqrt(jnp.maximum(rest, 1e-37)) * admit * x


def block_dots(smoothed, blocks, store):
    wide = blocks.shape[1]
    for q in range(blocks.shape[0]):
        at = slice(q * wide, (q + 1) * wide)
        both = dot(smoothed[:, at], blocks[q])
        store(at, both[:, :wide], both[:, wide:])


def scan_kernel(
    inner, normed_own, normed_other, w_gate, conv, w_decay, b_decay, w_input, b_input, rate, offset, weight,
    mine_out, packed_out, ends_out, blocks, heads_shift,
    smoothed, pre_r, pre_i, shift, extended, gate, h_out, p_out, gated_h, gated_p, arrived,
):
    length, width = inner.shape
    run = length // SUB
    copies = [
        pltpu.make_async_copy(
            weight.at[:, pl.ds(q * width, width)], packed_out.at[pl.ds((q + 1) * width, width)], arrived.at[q]
        )
        for q in range(weight.shape[1] // width)
    ]
    for copy in copies:
        copy.start()
    taps = conv.shape[0]
    lead = (taps - 1) * SUB

    def picks(rows, base):
        r = lax.broadcasted_iota(jnp.int32, (rows, length), 0)
        c = lax.broadcasted_iota(jnp.int32, (rows, length), 1)
        return jnp.where(c == (r & (SUB - 1)) * run + (r >> 3) + base, 1.0, 0.0).astype(bf16)

    order = picks(length, 0)
    extended[pl.ds(lead, length), :] = dot(order, inner[...])
    extended[pl.ds(0, lead), :] = dot(picks(lead, 1 - taps), inner[...])

    smooth = extended[pl.ds(0, length), :] * conv[0:1, :]
    for tap in range(1, taps):
        smooth = smooth + extended[pl.ds(tap * SUB, length), :] * conv[tap : tap + 1, :]
    smoothed[...] = smooth.astype(bf16)

    heads, block = w_decay.shape[0], w_decay.shape[1]
    wide = blocks.shape[1]
    per = wide // block
    blocks[...] = jnp.zeros_like(blocks)
    for head in range(heads):
        q, i = head // per, (head % per) * block
        blocks[q, pl.ds(i, block), pl.ds(i, block)] = -w_decay[head]
        blocks[q, pl.ds(i, block), pl.ds(wide + i, block)] = -w_input[head]

    def store(at, r, i):
        pre_r[:, at] = r
        pre_i[:, at] = i

    block_dots(smoothed, blocks, store)

    part0 = offset[...].astype(bf16).astype(f32)
    part1 = (offset[...] - part0).astype(bf16).astype(f32)
    part2 = offset[...] - part0 - part1
    parts = jnp.concatenate([part0, part1, part2, jnp.zeros_like(part0)], axis=0).astype(bf16)
    moved = lax.dot_general(parts, order, (((1,), (1,)), ((), ())), preferred_element_type=f32).astype(bf16)
    r = lax.broadcasted_iota(jnp.int32, (4 * heads, width), 0)
    c = lax.broadcasted_iota(jnp.int32, (4 * heads, width), 1)
    spread = jnp.where((r & (heads - 1)) == (c >> 6), 1.0, 0.0).astype(bf16)
    shift[...] = lax.dot_general(moved, spread, (((0,), (0,)), ((), ())), preferred_element_type=f32)
    heads_shift[...] = shift[pl.ds(0, heads_shift.shape[0]), :]

    rows = 4 * SUB

    def scan_rows(i, carry, skip=0):
        h, p = carry
        at = pl.ds(pl.multiple_of(i * rows, rows), rows)
        decay, drive = gates(
            pre_r[at, :], pre_i[at, :], smoothed[at, :].astype(f32), b_decay[...], b_input[...], rate[...], shift[at, :]
        )
        known = lax.broadcasted_iota(jnp.int32, (SUB, width), 0) > 0
        for k in range(rows // SUB):
            a, b = decay[k * SUB : (k + 1) * SUB, :], drive[k * SUB : (k + 1) * SUB, :]
            if k < skip:
                a, b = jnp.where(known, a, 1.0), jnp.where(known, b, 0.0)
            h = a * h + b
            p = a * p
            here = pl.ds(pl.multiple_of(i * rows + k * SUB, SUB), SUB)
            h_out[here, :] = h
            p_out[here, :] = p
        return h, p

    start = (jnp.zeros((SUB, width), f32), jnp.ones((SUB, width), f32))
    h, p = start
    half, blocks_half = length // 2, length // rows // 2
    tp = lax.axis_index("tp")
    for c, (normed, place) in enumerate(((normed_own, tp), (normed_other, 1 - tp))):
        at = pl.ds(pl.multiple_of(place * half, half), half)
        gate[at, :] = dot(normed[...], w_gate[...]).astype(bf16)
        for i in range(c * blocks_half, (c + 1) * blocks_half):
            h, p = scan_rows(i, (h, p), 0 if i else taps - 1)
    each = length // 4
    for c in range(0, length, each):
        here = slice(c, c + each)
        g = jax.nn.gelu(dot(order[here], gate[...]))
        gated_h[here, :] = (h_out[here, :] * g).astype(bf16)
        gated_p[here, :] = (p_out[here, :] * g).astype(bf16)

    def back(gated, begin):
        t = lax.broadcasted_iota(jnp.int32, (half, length), 0) + begin
        c = lax.broadcasted_iota(jnp.int32, (half, length), 1)
        pick = jnp.where(t == (c & (SUB - 1)) * run + (c >> 3), 1.0, 0.0).astype(bf16)
        return dot(pick, gated[...]).astype(bf16)

    for i, gated in enumerate((gated_h, gated_p)):
        packed_out[pl.ds(i * half, half), :] = back(gated, (1 - tp) * half)
        mine_out[pl.ds(i * half, half), :] = back(gated, tp * half)
    for copy in copies:
        copy.wait()
    ends_out[0] = p
    ends_out[1] = h


def pack_kernel(
    inner, halo, conv, blocks, b_decay, b_input, rate, shift, ends, packed,
    small_out, packed_out, sent_out,
    near, smoothed, pre_r, pre_i,
):
    width = inner.shape[1]
    taps = conv.shape[0]
    near[pl.ds(0, HALO), :] = halo[...].astype(f32)
    near[pl.ds(HALO, HALO), :] = inner[pl.ds(0, 2 * HALO), :].astype(f32)[:HALO]
    smooth = near[pl.ds(HALO - taps + 1, HALO), :] * conv[0:1, :]
    for tap in range(1, taps):
        smooth = smooth + near[pl.ds(HALO - taps + 1 + tap, HALO), :] * conv[tap : tap + 1, :]
    smoothed[...] = jnp.concatenate([smooth, jnp.zeros_like(smooth)], axis=0).astype(bf16)

    def store(at, r, i):
        pre_r[:, at] = r[:HALO]
        pre_i[:, at] = i[:HALO]

    block_dots(smoothed, blocks, store)
    shifts = jnp.concatenate([shift[pl.ds(k * SUB, 1), :] for k in range(HALO)], axis=0)
    decay, drive = gates(
        pre_r[...], pre_i[...], smoothed[...].astype(f32)[:HALO], b_decay[...], b_input[...], rate[...], shifts
    )
    one, zero = jnp.ones((1, width), f32), jnp.zeros((1, width), f32)
    a_before, b_before, head_a, head_b = one, zero, [], []
    for k in range(taps - 1):
        a_k = decay[k : k + 1, :]
        a_before, b_before = a_before * a_k, a_k * b_before + drive[k : k + 1, :]
        head_a.append(a_before)
        head_b.append(b_before)
    runs_a, runs_b = [], []
    for s in range(SUB):
        runs_a.append(a_before)
        runs_b.append(b_before)
        a_s = ends[0, s : s + 1, :]
        a_before, b_before = a_before * a_s, a_s * b_before + ends[1, s : s + 1, :]
    pair = jnp.concatenate([a_before, b_before], axis=0)
    sent_out[...] = jnp.broadcast_to(pair[None], sent_out.shape)
    small = jnp.concatenate(runs_a + runs_b + head_a + head_b, axis=0)
    small = jnp.concatenate([small, jnp.zeros((SMALL - small.shape[0], width), f32)], axis=0)
    small_out[...] = small
    for i in range(PARTS):
        part = small.astype(bf16)
        packed_out[pl.ds(packed.shape[0] - (PARTS - i) * SMALL, SMALL), :] = part
        small = small - part.astype(f32)


def before_in(pieces, index):
    width = pieces[0].shape[1]
    a, b = jnp.ones((1, width), f32), jnp.zeros((1, width), f32)
    a_at, b_at = a, b
    for k, piece in enumerate(pieces):
        here = k == index
        a_at, b_at = jnp.where(here, a, a_at), jnp.where(here, b, b_at)
        a_k, b_k = piece[0:1], piece[1:2]
        a, b = a * a_k, a_k * b + b_k
    return (a_at, b_at), (a, b)


def plane_kernel(pieces, before_out, sent_out):
    index = lax.axis_index("sp_1") * lax.axis_size("sp_2") + lax.axis_index("sp_2")
    (a_at, b_at), (a, b) = before_in([pieces[k] for k in range(pieces.shape[0])], index)
    before = jnp.concatenate([a_at, b_at], axis=0)
    before_out[...] = before
    pair = jnp.concatenate([a, b], axis=0)
    partner = lax.axis_index("sp_0") * 2 + 1 - lax.axis_index("tp")
    for k in range(sent_out.shape[0]):
        sent_out[k] = jnp.where(k == partner, before, pair)


def out_kernel(pieces, before, small, mine, packed, received, out, theirs, block, gated_mine, gated_theirs, sent):
    half, width = out.shape[0], mine.shape[1]
    run = half // (SUB // 2)
    deep = pieces.shape[0] // 2
    at, tp = lax.axis_index("sp_0"), lax.axis_index("tp")
    is_one = tp == 1
    for k in range(deep):
        theirs[k] = jnp.where(is_one, pieces[2 * k], pieces[2 * k + 1])
    own = [jnp.where(is_one, pieces[2 * k + 1], pieces[2 * k]) for k in range(deep)]
    cols = out.shape[1] // width
    last = (cols + 1) * width
    their_small = sum(received[pl.ds(last + i * SMALL, SMALL), :].astype(f32) for i in range(PARTS))
    sides = (
        (own, before[...], small[...], mine, gated_mine),
        ([theirs[k] for k in range(deep)], theirs[at], their_small, received, gated_theirs),
    )
    row = lax.broadcasted_iota(jnp.int32, (run, width), 0) + tp * half
    for totals, near, steps, parts, gated in sides:
        (_, b_at), _ = before_in(totals, at)
        carried = near[0:1] * b_at + near[1:2]
        start = steps[:SUB] * carried + steps[SUB : 2 * SUB]
        start = jnp.where(is_one, start[SUB // 2 :], start[: SUB // 2])
        for u in range(SUB // 2):
            here, there = pl.ds(u * run, run), pl.ds(half + u * run, run)
            enter = start[u : u + 1]
            if u == 0:
                for k in range(HEADS):
                    a_k, b_k = steps[2 * SUB + k : 2 * SUB + k + 1], steps[2 * SUB + HEADS + k : 2 * SUB + HEADS + k + 1]
                    enter = jnp.where(row == k, a_k * carried + b_k, enter)
            gated[here, :] = (parts[here, :].astype(f32) + parts[there, :].astype(f32) * enter).astype(bf16)
    copies = []
    for q in range(cols):
        w = pl.ds((q + 1) * width, width)
        block[q] = (dot(gated_mine[...], packed[w, :]) + dot(gated_theirs[...], received[w, :])).astype(bf16)
        copies.append(pltpu.make_async_copy(block.at[q], out.at[:, pl.ds(q * width, width)], sent.at[q]))
        copies[q].start()
    for copy in copies:
        copy.wait()


VMEM = pl.BlockSpec(memory_space=pltpu.VMEM)


HBM = pl.BlockSpec(memory_space=pltpu.HBM)
PARTS = 3
SMALL = 32
HEADS = 3
LATER = 8


def call(kernel, inputs, out_shape, scratch=(), out_specs=None, aliases=None):
    run = pl.pallas_call(
        kernel,
        out_shape=out_shape,
        out_specs=out_specs or jax.tree.map(lambda _: VMEM, out_shape),
        scratch_shapes=list(scratch),
        compiler_params=pltpu.CompilerParams(vmem_limit_bytes=32 * 1024 * 1024),
        in_specs=[VMEM] * inputs[0] + [HBM] * inputs[1],
        input_output_aliases=aliases or {},
    )

    def place(i, a):
        return pltpu.with_memory_space_constraint(a, pltpu.VMEM if i < inputs[0] else pltpu.HBM)

    return lambda *args: run(*(place(i, a) for i, a in enumerate(args)))


def step(
    tokens,
    norm_gain,
    in_weight,
    gate_weight,
    conv_weight,
    decay_gate_weight,
    decay_gate_bias,
    input_gate_weight,
    input_gate_bias,
    channel_decay_rate,
    forgetting_offset,
    out_weight,
):
    half, features = tokens.shape
    length = 2 * half
    width = in_weight.shape[1]
    heads, block = decay_gate_weight.shape[:2]
    count = lax.axis_size(SP)
    plane = lax.axis_size(PLANE)
    deep = lax.axis_size("sp_0")
    S = jax.ShapeDtypeStruct

    swap = [(0, 1), (1, 0)]
    other = lax.ppermute(tokens, "tp", swap)

    row = lambda v: v.reshape(1, -1)
    later = (
        gate_weight, conv_weight, decay_gate_weight, row(decay_gate_bias),
        input_gate_weight, row(input_gate_bias), row(channel_decay_rate), forgetting_offset,
    )
    big = pltpu.VMEM
    like = lambda a: big(a.shape, a.dtype)
    square = big((length, width), f32)
    stats = [big((half, 128), f32), big((half, 128), f32)]
    gain = row(norm_gain)
    inner_own, normed_own, gain, w_in = call(
        own_tokens_kernel,
        (0, 3),
        (big((half, width), bf16), big((half, features), bf16), like(gain), like(in_weight)),
        scratch=[like(tokens), pltpu.SemaphoreType.DMA((3,)), *stats],
    )(gain, in_weight, tokens)
    inner, tail, normed_other, *held = call(
        other_tokens_kernel,
        (4, LATER),
        (
            big((length, width), bf16), big((HALO, width), bf16), big((half, features), bf16),
            *(like(a) for a in later),
        ),
        scratch=[pltpu.SemaphoreType.DMA((LATER,)), *stats],
    )(other, gain, w_in, inner_own, *later)
    w_gate, conv, w_decay, b_decay, w_input, b_input, rate, offset = held
    halo = lax.ppermute(tail, SP, [(s, s + 1) for s in range(count - 1)])
    taps = conv_weight.shape[0]
    cols = features // width
    packed_shape = big(((cols + 1) * width + PARTS * SMALL, width), bf16)
    half_square = big((length, width), bf16)
    mine, packed, ends, blocks, shift = call(
        scan_kernel,
        (11, 1),
        (
            half_square, packed_shape, big((2, SUB, width), f32),
            big((heads * block // 256, 256, 512), bf16), big((HALO * SUB, width), f32),
        ),
        scratch=[
            half_square, square, square, square,
            big((length + (taps - 1) * SUB, width), f32), half_square,
            square, square, half_square, half_square, pltpu.SemaphoreType.DMA((cols,)),
        ],
    )(
        inner, normed_own, normed_other, w_gate, conv, w_decay, b_decay, w_input, b_input, rate, offset, out_weight,
    )
    small, packed, sent = call(
        pack_kernel,
        (10, 0),
        (big((SMALL, width), f32), packed_shape, big((plane, 2, width), f32)),
        scratch=[
            big((2 * HALO, width), f32), big((2 * HALO, width), bf16),
            big((HALO, width), f32), big((HALO, width), f32),
        ],
        aliases={9: 1},
    )(inner, halo, conv, blocks, b_decay, b_input, rate, shift, ends, packed)
    received = lax.ppermute(packed, "tp", swap)
    pieces = lax.all_to_all(sent, PLANE, split_axis=0, concat_axis=0, tiled=True)
    before, sent = call(plane_kernel, (1, 0), (big((2, width), f32), big((2 * deep, 2, width), f32)))(pieces)
    pieces = lax.all_to_all(sent, ("sp_0", "tp"), split_axis=0, concat_axis=0, tiled=True)
    return call(
        out_kernel,
        (6, 0),
        S((half, features), bf16),
        scratch=(
            big((deep, 2, width), f32), big((cols, half, width), bf16),
            big((half, width), bf16), big((half, width), bf16), pltpu.SemaphoreType.DMA((cols,)),
        ),
        out_specs=HBM,
    )(pieces, before, small, mine, packed, received)


def solution(mesh):
    torus = Mesh(mesh.devices.reshape(8, 8, 4, mesh.shape["tp"]), SP_TP)
    placed = (
        P(SP_TP, None),
        P(),
        P(None, "tp"),
        P(None, "tp"),
        P(None, "tp"),
        P("tp", None, None),
        P("tp"),
        P("tp", None, None),
        P("tp"),
        P("tp"),
        P("tp", SP),
        P("tp", None),
    )
    return jax.shard_map(step, mesh=torus, in_specs=placed, out_specs=P(SP_TP, None), check_vma=False)
```

```python
import jax
import jax.numpy as jnp
from jax import lax
from jax.experimental import pallas as pl
from jax.experimental.pallas import tpu as pltpu
from jax.sharding import Mesh
from jax.sharding import PartitionSpec as P

SP = ("sp_0", "sp_1", "sp_2")
PLANE = ("sp_2", "sp_1")
SP_TP = ("sp_0", "sp_1", "sp_2", "tp")

EPSILON = 1e-05
SUB = 8
HALO = 8
f32, bf16 = jnp.float32, jnp.bfloat16


def dot(a, b):
    return jnp.dot(a, b, preferred_element_type=f32)


def norm_tokens(source, target, gain, middle, scale, ready=None, arrivals=()):
    half, features = source.shape
    step, lanes = 32, 128

    def tiles(r):
        return [source[r, t : t + lanes].astype(f32) for t in range(0, features, lanes)]

    def by_rows(one, first=0, last=half // step):
        def rows(i, _):
            one(pl.ds(pl.multiple_of(i * step, step), step))
            return 0

        lax.fori_loop(first, last, rows, 0)

    def over_features(stat):
        return jnp.broadcast_to(jnp.sum(stat[...], axis=1, keepdims=True) * (1.0 / features), stat.shape)

    def add_up(r):
        middle[r, :] = sum(tiles(r))

    each = half // step // max(1, len(arrivals))
    for i, arrival in enumerate(arrivals or (None,)):
        if arrival is not None:
            arrival.wait()
        by_rows(add_up, i * each, (i + 1) * each)
    middle[...] = over_features(middle)

    def add_squares(r):
        m = middle[r, :]
        scale[r, :] = sum((x - m) * (x - m) for x in tiles(r))

    by_rows(add_squares)
    scale[...] = lax.rsqrt(over_features(scale) + EPSILON)
    if ready is not None:
        ready.wait()

    def write(r):
        m, k = middle[r, :], scale[r, :]
        for t, x in zip(range(0, features, lanes), tiles(r)):
            target[r, t : t + lanes] = ((x - m) * k * gain[:, t : t + lanes]).astype(bf16)

    by_rows(write)


def fetch(stored, held, arrived, order):
    copies = [pltpu.make_async_copy(a, b, arrived.at[i]) for i, (a, b) in enumerate(zip(stored, held))]
    for i in order:
        copies[i].start()
    return copies


def own_tokens_kernel(gain_in, w_in_in, own_in, inner, normed, gain, w_in, own, arrived, middle, scale):
    rows = own.shape[0] // 2
    halves = [pl.ds(i * rows, rows) for i in range(2)]
    copies = fetch(
        (gain_in, w_in_in, *(own_in.at[r] for r in halves)), (gain, w_in, *(own.at[r] for r in halves)), arrived, (2, 3, 0, 1)
    )
    norm_tokens(own, normed, gain, middle, scale, copies[0], copies[2:])
    copies[1].wait()
    inner[...] = dot(normed[...], w_in[...]).astype(bf16)


def other_tokens_kernel(other, gain, w_in, inner_own, *refs):
    stored, refs = refs[:LATER], refs[LATER:]
    inner, tail, normed, *held = refs[: 3 + LATER]
    arrived, middle, scale = refs[3 + LATER :]
    copies = fetch(stored, held, arrived, range(LATER))
    half = other.shape[0]
    tp = lax.axis_index("tp")
    norm_tokens(other, normed, gain, middle, scale)
    inner[pl.ds(pl.multiple_of(tp * half, half), half), :] = inner_own[...]
    there = pl.ds(pl.multiple_of((1 - tp) * half, half), half)
    inner[there, :] = dot(normed[...], w_in[...]).astype(bf16)
    tail[...] = inner[pl.ds(2 * half - 2 * HALO, 2 * HALO), :].astype(f32)[HALO:].astype(bf16)
    for copy in copies:
        copy.wait()


def gates(minus_r, minus_i, x, b_decay, b_input, rate, shift):
    retain = 1.0 / (1.0 + jnp.exp(minus_r - b_decay))
    admit = 1.0 / (1.0 + jnp.exp(minus_i - b_input))
    log_decay = retain * (-8.0 * rate) + shift
    decay = jnp.exp(log_decay)
    rest = jnp.tanh(log_decay) * (-1.0 - decay * decay)
    return decay, rest * lax.rsqrt(jnp.maximum(rest, 1e-37)) * admit * x


def block_dots(smoothed, blocks, store):
    wide = blocks.shape[1]
    for q in range(blocks.shape[0]):
        at = slice(q * wide, (q + 1) * wide)
        both = dot(smoothed[:, at], blocks[q])
        store(at, both[:, :wide], both[:, wide:])


def scan_kernel(
    inner, normed_own, normed_other, w_gate, conv, w_decay, b_decay, w_input, b_input, rate, offset, weight,
    mine_out, packed_out, ends_out, blocks, heads_shift,
    smoothed, pre_r, pre_i, shift, extended, gate, h_out, p_out, gated_h, gated_p, arrived,
):
    length, width = inner.shape
    run = length // SUB
    copies = [
        pltpu.make_async_copy(
            weight.at[:, pl.ds(q * width, width)], packed_out.at[pl.ds((q + 1) * width, width)], arrived.at[q]
        )
        for q in range(weight.shape[1] // width)
    ]
    for copy in copies:
        copy.start()
    taps = conv.shape[0]
    lead = (taps - 1) * SUB

    def picks(rows, base):
        r = lax.broadcasted_iota(jnp.int32, (rows, length), 0)
        c = lax.broadcasted_iota(jnp.int32, (rows, length), 1)
        return jnp.where(c == (r & (SUB - 1)) * run + (r >> 3) + base, 1.0, 0.0).astype(bf16)

    order = picks(length, 0)
    extended[pl.ds(lead, length), :] = dot(order, inner[...])
    extended[pl.ds(0, lead), :] = dot(picks(lead, 1 - taps), inner[...])

    smooth = extended[pl.ds(0, length), :] * conv[0:1, :]
    for tap in range(1, taps):
        smooth = smooth + extended[pl.ds(tap * SUB, length), :] * conv[tap : tap + 1, :]
    smoothed[...] = smooth.astype(bf16)

    heads, block = w_decay.shape[0], w_decay.shape[1]
    wide = blocks.shape[1]
    per = wide // block
    blocks[...] = jnp.zeros_like(blocks)
    for head in range(heads):
        q, i = head // per, (head % per) * block
        blocks[q, pl.ds(i, block), pl.ds(i, block)] = -w_decay[head]
        blocks[q, pl.ds(i, block), pl.ds(wide + i, block)] = -w_input[head]

    def store(at, r, i):
        pre_r[:, at] = r
        pre_i[:, at] = i

    block_dots(smoothed, blocks, store)

    part0 = offset[...].astype(bf16).astype(f32)
    part1 = (offset[...] - part0).astype(bf16).astype(f32)
    part2 = offset[...] - part0 - part1
    parts = jnp.concatenate([part0, part1, part2, jnp.zeros_like(part0)], axis=0).astype(bf16)
    moved = lax.dot_general(parts, order, (((1,), (1,)), ((), ())), preferred_element_type=f32).astype(bf16)
    r = lax.broadcasted_iota(jnp.int32, (4 * heads, width), 0)
    c = lax.broadcasted_iota(jnp.int32, (4 * heads, width), 1)
    spread = jnp.where((r & (heads - 1)) == (c >> 6), 1.0, 0.0).astype(bf16)
    shift[...] = lax.dot_general(moved, spread, (((0,), (0,)), ((), ())), preferred_element_type=f32)
    heads_shift[...] = shift[pl.ds(0, heads_shift.shape[0]), :]

    rows = 4 * SUB

    def scan_rows(i, carry, skip=0):
        h, p = carry
        at = pl.ds(pl.multiple_of(i * rows, rows), rows)
        decay, drive = gates(
            pre_r[at, :], pre_i[at, :], smoothed[at, :].astype(f32), b_decay[...], b_input[...], rate[...], shift[at, :]
        )
        known = lax.broadcasted_iota(jnp.int32, (SUB, width), 0) > 0
        for k in range(rows // SUB):
            a, b = decay[k * SUB : (k + 1) * SUB, :], drive[k * SUB : (k + 1) * SUB, :]
            if k < skip:
                a, b = jnp.where(known, a, 1.0), jnp.where(known, b, 0.0)
            h = a * h + b
            p = a * p
            here = pl.ds(pl.multiple_of(i * rows + k * SUB, SUB), SUB)
            h_out[here, :] = h
            p_out[here, :] = p
        return h, p

    start = (jnp.zeros((SUB, width), f32), jnp.ones((SUB, width), f32))
    h, p = start
    half, blocks_half = length // 2, length // rows // 2
    tp = lax.axis_index("tp")
    for c, (normed, place) in enumerate(((normed_own, tp), (normed_other, 1 - tp))):
        at = pl.ds(pl.multiple_of(place * half, half), half)
        gate[at, :] = dot(normed[...], w_gate[...]).astype(bf16)
        for i in range(c * blocks_half, (c + 1) * blocks_half):
            h, p = scan_rows(i, (h, p), 0 if i else taps - 1)
    each = length // 4
    for c in range(0, length, each):
        here = slice(c, c + each)
        g = jax.nn.gelu(dot(order[here], gate[...]))
        gated_h[here, :] = (h_out[here, :] * g).astype(bf16)
        gated_p[here, :] = (p_out[here, :] * g).astype(bf16)

    def back(gated, begin):
        t = lax.broadcasted_iota(jnp.int32, (half, length), 0) + begin
        c = lax.broadcasted_iota(jnp.int32, (half, length), 1)
        pick = jnp.where(t == (c & (SUB - 1)) * run + (c >> 3), 1.0, 0.0).astype(bf16)
        return dot(pick, gated[...]).astype(bf16)

    for i, gated in enumerate((gated_h, gated_p)):
        packed_out[pl.ds(i * half, half), :] = back(gated, (1 - tp) * half)
        mine_out[pl.ds(i * half, half), :] = back(gated, tp * half)
    for copy in copies:
        copy.wait()
    ends_out[0] = p
    ends_out[1] = h


def pack_kernel(
    inner, halo, conv, blocks, b_decay, b_input, rate, shift, ends, packed,
    small_out, packed_out, sent_out,
    near, smoothed, pre_r, pre_i,
):
    width = inner.shape[1]
    taps = conv.shape[0]
    near[pl.ds(0, HALO), :] = halo[...].astype(f32)
    near[pl.ds(HALO, HALO), :] = inner[pl.ds(0, 2 * HALO), :].astype(f32)[:HALO]
    smooth = near[pl.ds(HALO - taps + 1, HALO), :] * conv[0:1, :]
    for tap in range(1, taps):
        smooth = smooth + near[pl.ds(HALO - taps + 1 + tap, HALO), :] * conv[tap : tap + 1, :]
    smoothed[...] = jnp.concatenate([smooth, jnp.zeros_like(smooth)], axis=0).astype(bf16)

    def store(at, r, i):
        pre_r[:, at] = r[:HALO]
        pre_i[:, at] = i[:HALO]

    block_dots(smoothed, blocks, store)
    shifts = jnp.concatenate([shift[pl.ds(k * SUB, 1), :] for k in range(HALO)], axis=0)
    decay, drive = gates(
        pre_r[...], pre_i[...], smoothed[...].astype(f32)[:HALO], b_decay[...], b_input[...], rate[...], shifts
    )
    one, zero = jnp.ones((1, width), f32), jnp.zeros((1, width), f32)
    a_before, b_before, head_a, head_b = one, zero, [], []
    for k in range(taps - 1):
        a_k = decay[k : k + 1, :]
        a_before, b_before = a_before * a_k, a_k * b_before + drive[k : k + 1, :]
        head_a.append(a_before)
        head_b.append(b_before)
    runs_a, runs_b = [], []
    for s in range(SUB):
        runs_a.append(a_before)
        runs_b.append(b_before)
        a_s = ends[0, s : s + 1, :]
        a_before, b_before = a_before * a_s, a_s * b_before + ends[1, s : s + 1, :]
    pair = jnp.concatenate([a_before, b_before], axis=0)
    sent_out[...] = jnp.broadcast_to(pair[None], sent_out.shape)
    small = jnp.concatenate(runs_a + runs_b + head_a + head_b, axis=0)
    small = jnp.concatenate([small, jnp.zeros((SMALL - small.shape[0], width), f32)], axis=0)
    small_out[...] = small
    for i in range(PARTS):
        part = small.astype(bf16)
        packed_out[pl.ds(packed.shape[0] - (PARTS - i) * SMALL, SMALL), :] = part
        small = small - part.astype(f32)


def before_in(pieces, index):
    width = pieces[0].shape[1]
    a, b = jnp.ones((1, width), f32), jnp.zeros((1, width), f32)
    a_at, b_at = a, b
    for k, piece in enumerate(pieces):
        here = k == index
        a_at, b_at = jnp.where(here, a, a_at), jnp.where(here, b, b_at)
        a_k, b_k = piece[0:1], piece[1:2]
        a, b = a * a_k, a_k * b + b_k
    return (a_at, b_at), (a, b)


def plane_kernel(pieces, before_out, sent_out):
    index = lax.axis_index("sp_1") * lax.axis_size("sp_2") + lax.axis_index("sp_2")
    wide, high = lax.axis_size("sp_2"), lax.axis_size("sp_1")
    in_order = [pieces[k % wide * high + k // wide] for k in range(pieces.shape[0])]
    (a_at, b_at), (a, b) = before_in(in_order, index)
    before = jnp.concatenate([a_at, b_at], axis=0)
    before_out[...] = before
    pair = jnp.concatenate([a, b], axis=0)
    partner = (1 - lax.axis_index("tp")) * lax.axis_size("sp_0") + lax.axis_index("sp_0")
    for k in range(sent_out.shape[0]):
        sent_out[k] = jnp.where(k == partner, before, pair)


def out_kernel(pieces, before, small, mine, packed, received, out, theirs, block, gated_mine, gated_theirs, sent):
    half, width = out.shape[0], mine.shape[1]
    run = half // (SUB // 2)
    deep = pieces.shape[0] // 2
    at, tp = lax.axis_index("sp_0"), lax.axis_index("tp")
    is_one = tp == 1
    for k in range(deep):
        theirs[k] = jnp.where(is_one, pieces[k], pieces[deep + k])
    own = [jnp.where(is_one, pieces[deep + k], pieces[k]) for k in range(deep)]
    cols = out.shape[1] // width
    last = (cols + 1) * width
    their_small = sum(received[pl.ds(last + i * SMALL, SMALL), :].astype(f32) for i in range(PARTS))
    sides = (
        (own, before[...], small[...], mine, gated_mine),
        ([theirs[k] for k in range(deep)], theirs[at], their_small, received, gated_theirs),
    )
    row = lax.broadcasted_iota(jnp.int32, (run, width), 0) + tp * half
    for totals, near, steps, parts, gated in sides:
        (_, b_at), _ = before_in(totals, at)
        carried = near[0:1] * b_at + near[1:2]
        start = steps[:SUB] * carried + steps[SUB : 2 * SUB]
        start = jnp.where(is_one, start[SUB // 2 :], start[: SUB // 2])
        for u in range(SUB // 2):
            here, there = pl.ds(u * run, run), pl.ds(half + u * run, run)
            enter = start[u : u + 1]
            if u == 0:
                for k in range(HEADS):
                    a_k, b_k = steps[2 * SUB + k : 2 * SUB + k + 1], steps[2 * SUB + HEADS + k : 2 * SUB + HEADS + k + 1]
                    enter = jnp.where(row == k, a_k * carried + b_k, enter)
            gated[here, :] = (parts[here, :].astype(f32) + parts[there, :].astype(f32) * enter).astype(bf16)
    copies = []
    narrow = block.shape[2]
    for q in range(cols):
        w = pl.ds((q + 1) * width, width)
        for i in range(width // narrow):
            part, k = pl.ds(i * narrow, narrow), q * (width // narrow) + i
            block[k] = (dot(gated_mine[...], packed[w, part]) + dot(gated_theirs[...], received[w, part])).astype(bf16)
            copies.append(pltpu.make_async_copy(block.at[k], out.at[:, pl.ds(k * narrow, narrow)], sent.at[k]))
            copies[k].start()
    for copy in copies:
        copy.wait()


VMEM = pl.BlockSpec(memory_space=pltpu.VMEM)


HBM = pl.BlockSpec(memory_space=pltpu.HBM)
PARTS = 3
SMALL = 32
HEADS = 3
LATER = 8


def call(kernel, inputs, out_shape, scratch=(), out_specs=None, aliases=None):
    run = pl.pallas_call(
        kernel,
        out_shape=out_shape,
        out_specs=out_specs or jax.tree.map(lambda _: VMEM, out_shape),
        scratch_shapes=list(scratch),
        compiler_params=pltpu.CompilerParams(vmem_limit_bytes=32 * 1024 * 1024),
        in_specs=[VMEM] * inputs[0] + [HBM] * inputs[1],
        input_output_aliases=aliases or {},
    )

    def place(i, a):
        return pltpu.with_memory_space_constraint(a, pltpu.VMEM if i < inputs[0] else pltpu.HBM)

    return lambda *args: run(*(place(i, a) for i, a in enumerate(args)))


def step(
    tokens,
    norm_gain,
    in_weight,
    gate_weight,
    conv_weight,
    decay_gate_weight,
    decay_gate_bias,
    input_gate_weight,
    input_gate_bias,
    channel_decay_rate,
    forgetting_offset,
    out_weight,
):
    half, features = tokens.shape
    length = 2 * half
    width = in_weight.shape[1]
    heads, block = decay_gate_weight.shape[:2]
    count = lax.axis_size(SP)
    plane = lax.axis_size(PLANE)
    deep = lax.axis_size("sp_0")
    S = jax.ShapeDtypeStruct

    swap = [(0, 1), (1, 0)]
    other = lax.ppermute(tokens, "tp", swap)

    row = lambda v: v.reshape(1, -1)
    later = (
        gate_weight, conv_weight, decay_gate_weight, row(decay_gate_bias),
        input_gate_weight, row(input_gate_bias), row(channel_decay_rate), forgetting_offset,
    )
    big = pltpu.VMEM
    like = lambda a: big(a.shape, a.dtype)
    square = big((length, width), f32)
    stats = [big((half, 128), f32), big((half, 128), f32)]
    gain = row(norm_gain)
    inner_own, normed_own, gain, w_in = call(
        own_tokens_kernel,
        (0, 3),
        (big((half, width), bf16), big((half, features), bf16), like(gain), like(in_weight)),
        scratch=[like(tokens), pltpu.SemaphoreType.DMA((4,)), *stats],
    )(gain, in_weight, tokens)
    inner, tail, normed_other, *held = call(
        other_tokens_kernel,
        (4, LATER),
        (
            big((length, width), bf16), big((HALO, width), bf16), big((half, features), bf16),
            *(like(a) for a in later),
        ),
        scratch=[pltpu.SemaphoreType.DMA((LATER,)), *stats],
    )(other, gain, w_in, inner_own, *later)
    w_gate, conv, w_decay, b_decay, w_input, b_input, rate, offset = held
    halo = lax.ppermute(tail, SP, [(s, s + 1) for s in range(count - 1)])
    taps = conv_weight.shape[0]
    cols = features // width
    packed_shape = big(((cols + 1) * width + PARTS * SMALL, width), bf16)
    half_square = big((length, width), bf16)
    mine, packed, ends, blocks, shift = call(
        scan_kernel,
        (11, 1),
        (
            half_square, packed_shape, big((2, SUB, width), f32),
            big((heads * block // 256, 256, 512), bf16), big((HALO * SUB, width), f32),
        ),
        scratch=[
            half_square, square, square, square,
            big((length + (taps - 1) * SUB, width), f32), half_square,
            square, square, half_square, half_square, pltpu.SemaphoreType.DMA((cols,)),
        ],
    )(
        inner, normed_own, normed_other, w_gate, conv, w_decay, b_decay, w_input, b_input, rate, offset, out_weight,
    )
    small, packed, sent = call(
        pack_kernel,
        (10, 0),
        (big((SMALL, width), f32), packed_shape, big((plane, 2, width), f32)),
        scratch=[
            big((2 * HALO, width), f32), big((2 * HALO, width), bf16),
            big((HALO, width), f32), big((HALO, width), f32),
        ],
        aliases={9: 1},
    )(inner, halo, conv, blocks, b_decay, b_input, rate, shift, ends, packed)
    received = lax.ppermute(packed, "tp", swap)
    pieces = lax.all_to_all(sent, PLANE, split_axis=0, concat_axis=0, tiled=True)
    before, sent = call(plane_kernel, (1, 0), (big((2, width), f32), big((2 * deep, 2, width), f32)))(pieces)
    pieces = lax.all_to_all(sent, ("tp", "sp_0"), split_axis=0, concat_axis=0, tiled=True)
    return call(
        out_kernel,
        (6, 0),
        S((half, features), bf16),
        scratch=(
            big((deep, 2, width), f32), big((cols, half, width), bf16),
            big((half, width), bf16), big((half, width), bf16), pltpu.SemaphoreType.DMA((cols,)),
        ),
        out_specs=HBM,
    )(pieces, before, small, mine, packed, received)


def solution(mesh):
    torus = Mesh(mesh.devices.reshape(8, 8, 4, mesh.shape["tp"]), SP_TP)
    placed = (
        P(SP_TP, None),
        P(),
        P(None, "tp"),
        P(None, "tp"),
        P(None, "tp"),
        P("tp", None, None),
        P("tp"),
        P("tp", None, None),
        P("tp"),
        P("tp"),
        P("tp", SP),
        P("tp", None),
    )
    return jax.shard_map(step, mesh=torus, in_specs=placed, out_specs=P(SP_TP, None), check_vma=False)
```

```python
import jax
import jax.numpy as jnp
from jax import lax
from jax.experimental import pallas as pl
from jax.experimental.pallas import tpu as pltpu
from jax.sharding import Mesh
from jax.sharding import PartitionSpec as P

SP = ("sp_0", "sp_1", "sp_2")
PLANE = ("sp_2", "sp_1")
SP_TP = ("sp_0", "sp_1", "sp_2", "tp")

EPSILON = 1e-05
SUB = 8
HALO = 8
f32, bf16 = jnp.float32, jnp.bfloat16


def dot(a, b):
    return jnp.dot(a, b, preferred_element_type=f32)


def norm_tokens(source, target, gain, middle, scale, ready=None, arrivals=()):
    half, features = source.shape
    step, lanes = 32, 128

    def tiles(r):
        return [source[r, t : t + lanes].astype(f32) for t in range(0, features, lanes)]

    def by_rows(one, first=0, last=half // step):
        def rows(i, _):
            one(pl.ds(pl.multiple_of(i * step, step), step))
            return 0

        lax.fori_loop(first, last, rows, 0)

    def over_features(stat):
        return jnp.broadcast_to(jnp.sum(stat[...], axis=1, keepdims=True) * (1.0 / features), stat.shape)

    def add_up(r):
        middle[r, :] = sum(tiles(r))

    each = half // step // max(1, len(arrivals))
    for i, arrival in enumerate(arrivals or (None,)):
        if arrival is not None:
            arrival.wait()
        by_rows(add_up, i * each, (i + 1) * each)
    middle[...] = over_features(middle)

    def add_squares(r):
        m = middle[r, :]
        scale[r, :] = sum((x - m) * (x - m) for x in tiles(r))

    by_rows(add_squares)
    scale[...] = lax.rsqrt(over_features(scale) + EPSILON)
    if ready is not None:
        ready.wait()

    def write(r):
        m, k = middle[r, :], scale[r, :]
        for t, x in zip(range(0, features, lanes), tiles(r)):
            target[r, t : t + lanes] = ((x - m) * k * gain[:, t : t + lanes]).astype(bf16)

    by_rows(write)


def fetch(stored, held, arrived, order):
    copies = [pltpu.make_async_copy(a, b, arrived.at[i]) for i, (a, b) in enumerate(zip(stored, held))]
    for i in order:
        copies[i].start()
    return copies


def own_tokens_kernel(gain_in, w_in_in, own_in, inner, normed, gain, w_in, own, arrived, middle, scale):
    rows = own.shape[0] // 2
    halves = [pl.ds(i * rows, rows) for i in range(2)]
    copies = fetch(
        (gain_in, w_in_in, *(own_in.at[r] for r in halves)), (gain, w_in, *(own.at[r] for r in halves)), arrived, (2, 3, 0, 1)
    )
    norm_tokens(own, normed, gain, middle, scale, copies[0], copies[2:])
    copies[1].wait()
    inner[...] = dot(normed[...], w_in[...]).astype(bf16)


def other_tokens_kernel(other, gain, w_in, inner_own, *refs):
    stored, refs = refs[:LATER], refs[LATER:]
    inner, tail, normed, *held = refs[: 3 + LATER]
    arrived, middle, scale = refs[3 + LATER :]
    copies = fetch(stored, held, arrived, range(LATER))
    half = other.shape[0]
    tp = lax.axis_index("tp")
    norm_tokens(other, normed, gain, middle, scale)
    inner[pl.ds(pl.multiple_of(tp * half, half), half), :] = inner_own[...]
    there = pl.ds(pl.multiple_of((1 - tp) * half, half), half)
    inner[there, :] = dot(normed[...], w_in[...]).astype(bf16)
    tail[...] = inner[pl.ds(2 * half - 2 * HALO, 2 * HALO), :].astype(f32)[HALO:].astype(bf16)
    for copy in copies:
        copy.wait()


def gates(minus_r, minus_i, x, b_decay, b_input, rate, shift):
    retain = 1.0 / (1.0 + jnp.exp(minus_r - b_decay))
    admit = 1.0 / (1.0 + jnp.exp(minus_i - b_input))
    log_decay = retain * (-8.0 * rate) + shift
    decay = jnp.exp(log_decay)
    rest = jnp.tanh(log_decay) * (-1.0 - decay * decay)
    return decay, rest * lax.rsqrt(jnp.maximum(rest, 1e-37)) * admit * x


def block_dots(smoothed, blocks, store):
    wide = blocks.shape[1]
    for q in range(blocks.shape[0]):
        at = slice(q * wide, (q + 1) * wide)
        both = dot(smoothed[:, at], blocks[q])
        store(at, both[:, :wide], both[:, wide:])


def scan_kernel(
    inner, normed_own, normed_other, w_gate, conv, w_decay, b_decay, w_input, b_input, rate, offset, weight,
    mine_out, packed_out, ends_out, blocks, heads_shift,
    smoothed, pre_r, pre_i, shift, extended, gate, h_out, p_out, gated_h, gated_p, arrived,
):
    length, width = inner.shape
    run = length // SUB
    copies = [
        pltpu.make_async_copy(
            weight.at[:, pl.ds(q * width, width)], packed_out.at[pl.ds((q + 1) * width, width)], arrived.at[q]
        )
        for q in range(weight.shape[1] // width)
    ]
    for copy in copies:
        copy.start()
    taps = conv.shape[0]
    lead = (taps - 1) * SUB

    def picks(rows, base):
        r = lax.broadcasted_iota(jnp.int32, (rows, length), 0)
        c = lax.broadcasted_iota(jnp.int32, (rows, length), 1)
        return jnp.where(c == (r & (SUB - 1)) * run + (r >> 3) + base, 1.0, 0.0).astype(bf16)

    order = picks(length, 0)
    extended[pl.ds(lead, length), :] = dot(order, inner[...])
    extended[pl.ds(0, lead), :] = dot(picks(lead, 1 - taps), inner[...])

    smooth = extended[pl.ds(0, length), :] * conv[0:1, :]
    for tap in range(1, taps):
        smooth = smooth + extended[pl.ds(tap * SUB, length), :] * conv[tap : tap + 1, :]
    smoothed[...] = smooth.astype(bf16)

    heads, block = w_decay.shape[0], w_decay.shape[1]
    wide = blocks.shape[1]
    per = wide // block
    blocks[...] = jnp.zeros_like(blocks)
    for head in range(heads):
        q, i = head // per, (head % per) * block
        blocks[q, pl.ds(i, block), pl.ds(i, block)] = -w_decay[head]
        blocks[q, pl.ds(i, block), pl.ds(wide + i, block)] = -w_input[head]

    def store(at, r, i):
        pre_r[:, at] = r
        pre_i[:, at] = i

    block_dots(smoothed, blocks, store)

    part0 = offset[...].astype(bf16).astype(f32)
    part1 = (offset[...] - part0).astype(bf16).astype(f32)
    part2 = offset[...] - part0 - part1
    parts = jnp.concatenate([part0, part1, part2, jnp.zeros_like(part0)], axis=0).astype(bf16)
    moved = lax.dot_general(parts, order, (((1,), (1,)), ((), ())), preferred_element_type=f32).astype(bf16)
    r = lax.broadcasted_iota(jnp.int32, (4 * heads, width), 0)
    c = lax.broadcasted_iota(jnp.int32, (4 * heads, width), 1)
    spread = jnp.where((r & (heads - 1)) == (c >> 6), 1.0, 0.0).astype(bf16)
    shift[...] = lax.dot_general(moved, spread, (((0,), (0,)), ((), ())), preferred_element_type=f32)
    heads_shift[...] = shift[pl.ds(0, heads_shift.shape[0]), :]

    rows = 4 * SUB

    def scan_rows(i, carry, skip=0):
        h, p = carry
        at = pl.ds(pl.multiple_of(i * rows, rows), rows)
        decay, drive = gates(
            pre_r[at, :], pre_i[at, :], smoothed[at, :].astype(f32), b_decay[...], b_input[...], rate[...], shift[at, :]
        )
        known = lax.broadcasted_iota(jnp.int32, (SUB, width), 0) > 0
        for k in range(rows // SUB):
            a, b = decay[k * SUB : (k + 1) * SUB, :], drive[k * SUB : (k + 1) * SUB, :]
            if k < skip:
                a, b = jnp.where(known, a, 1.0), jnp.where(known, b, 0.0)
            h = a * h + b
            p = a * p
            here = pl.ds(pl.multiple_of(i * rows + k * SUB, SUB), SUB)
            h_out[here, :] = h
            p_out[here, :] = p
        return h, p

    start = (jnp.zeros((SUB, width), f32), jnp.ones((SUB, width), f32))
    h, p = start
    half, blocks_half = length // 2, length // rows // 2
    tp = lax.axis_index("tp")
    for c, (normed, place) in enumerate(((normed_own, tp), (normed_other, 1 - tp))):
        at = pl.ds(pl.multiple_of(place * half, half), half)
        gate[at, :] = dot(normed[...], w_gate[...]).astype(bf16)
        for i in range(c * blocks_half, (c + 1) * blocks_half):
            h, p = scan_rows(i, (h, p), 0 if i else taps - 1)
    each = length // 4
    for c in range(0, length, each):
        here = slice(c, c + each)
        g = jax.nn.gelu(dot(order[here], gate[...]))
        gated_h[here, :] = (h_out[here, :] * g).astype(bf16)
        gated_p[here, :] = (p_out[here, :] * g).astype(bf16)

    def back(gated, begin):
        t = lax.broadcasted_iota(jnp.int32, (half, length), 0) + begin
        c = lax.broadcasted_iota(jnp.int32, (half, length), 1)
        pick = jnp.where(t == (c & (SUB - 1)) * run + (c >> 3), 1.0, 0.0).astype(bf16)
        return dot(pick, gated[...]).astype(bf16)

    for i, gated in enumerate((gated_h, gated_p)):
        packed_out[pl.ds(i * half, half), :] = back(gated, (1 - tp) * half)
        mine_out[pl.ds(i * half, half), :] = back(gated, tp * half)
    for copy in copies:
        copy.wait()
    ends_out[0] = p
    ends_out[1] = h


def pack_kernel(
    inner, halo, conv, blocks, b_decay, b_input, rate, shift, ends, packed,
    small_out, packed_out, sent_out,
    near, smoothed, pre_r, pre_i,
):
    width = inner.shape[1]
    taps = conv.shape[0]
    near[pl.ds(0, HALO), :] = halo[...].astype(f32)
    near[pl.ds(HALO, HALO), :] = inner[pl.ds(0, 2 * HALO), :].astype(f32)[:HALO]
    smooth = near[pl.ds(HALO - taps + 1, HALO), :] * conv[0:1, :]
    for tap in range(1, taps):
        smooth = smooth + near[pl.ds(HALO - taps + 1 + tap, HALO), :] * conv[tap : tap + 1, :]
    smoothed[...] = jnp.concatenate([smooth, jnp.zeros_like(smooth)], axis=0).astype(bf16)

    def store(at, r, i):
        pre_r[:, at] = r[:HALO]
        pre_i[:, at] = i[:HALO]

    block_dots(smoothed, blocks, store)
    shifts = jnp.concatenate([shift[pl.ds(k * SUB, 1), :] for k in range(HALO)], axis=0)
    decay, drive = gates(
        pre_r[...], pre_i[...], smoothed[...].astype(f32)[:HALO], b_decay[...], b_input[...], rate[...], shifts
    )
    one, zero = jnp.ones((1, width), f32), jnp.zeros((1, width), f32)
    a_before, b_before, head_a, head_b = one, zero, [], []
    for k in range(taps - 1):
        a_k = decay[k : k + 1, :]
        a_before, b_before = a_before * a_k, a_k * b_before + drive[k : k + 1, :]
        head_a.append(a_before)
        head_b.append(b_before)
    runs_a, runs_b = [], []
    for s in range(SUB):
        runs_a.append(a_before)
        runs_b.append(b_before)
        a_s = ends[0, s : s + 1, :]
        a_before, b_before = a_before * a_s, a_s * b_before + ends[1, s : s + 1, :]
    pair = jnp.concatenate([a_before, b_before], axis=0)
    sent_out[...] = jnp.broadcast_to(pair[None], sent_out.shape)
    small = jnp.concatenate(runs_a + runs_b + head_a + head_b, axis=0)
    small = jnp.concatenate([small, jnp.zeros((SMALL - small.shape[0], width), f32)], axis=0)
    small_out[...] = small
    for i in range(PARTS):
        part = small.astype(bf16)
        packed_out[pl.ds(packed.shape[0] - (PARTS - i) * SMALL, SMALL), :] = part
        small = small - part.astype(f32)


def before_in(pieces, index):
    width = pieces[0].shape[1]
    a, b = jnp.ones((1, width), f32), jnp.zeros((1, width), f32)
    a_at, b_at = a, b
    for k, piece in enumerate(pieces):
        here = k == index
        a_at, b_at = jnp.where(here, a, a_at), jnp.where(here, b, b_at)
        a_k, b_k = piece[0:1], piece[1:2]
        a, b = a * a_k, a_k * b + b_k
    return (a_at, b_at), (a, b)


def plane_kernel(pieces, before_out, sent_out):
    index = lax.axis_index("sp_1") * lax.axis_size("sp_2") + lax.axis_index("sp_2")
    wide, high = lax.axis_size("sp_2"), lax.axis_size("sp_1")
    in_order = [pieces[k % wide * high + k // wide] for k in range(pieces.shape[0])]
    (a_at, b_at), (a, b) = before_in(in_order, index)
    before = jnp.concatenate([a_at, b_at], axis=0)
    before_out[...] = before
    pair = jnp.concatenate([a, b], axis=0)
    partner = lax.axis_index("sp_0") * 2 + 1 - lax.axis_index("tp")
    for k in range(sent_out.shape[0]):
        sent_out[k] = jnp.where(k == partner, before, pair)


def out_kernel(pieces, before, small, mine, packed, received, out, theirs, block, gated_mine, gated_theirs, sent):
    half, width = out.shape[0], mine.shape[1]
    run = half // (SUB // 2)
    deep = pieces.shape[0] // 2
    at, tp = lax.axis_index("sp_0"), lax.axis_index("tp")
    is_one = tp == 1
    for k in range(deep):
        theirs[k] = jnp.where(is_one, pieces[2 * k], pieces[2 * k + 1])
    own = [jnp.where(is_one, pieces[2 * k + 1], pieces[2 * k]) for k in range(deep)]
    cols = out.shape[1] // width
    last = (cols + 1) * width
    their_small = sum(received[pl.ds(last + i * SMALL, SMALL), :].astype(f32) for i in range(PARTS))
    sides = (
        (own, before[...], small[...], mine, gated_mine),
        ([theirs[k] for k in range(deep)], theirs[at], their_small, received, gated_theirs),
    )
    row = lax.broadcasted_iota(jnp.int32, (run, width), 0) + tp * half
    for totals, near, steps, parts, gated in sides:
        (_, b_at), _ = before_in(totals, at)
        carried = near[0:1] * b_at + near[1:2]
        start = steps[:SUB] * carried + steps[SUB : 2 * SUB]
        start = jnp.where(is_one, start[SUB // 2 :], start[: SUB // 2])
        for u in range(SUB // 2):
            here, there = pl.ds(u * run, run), pl.ds(half + u * run, run)
            enter = start[u : u + 1]
            if u == 0:
                for k in range(HEADS):
                    a_k, b_k = steps[2 * SUB + k : 2 * SUB + k + 1], steps[2 * SUB + HEADS + k : 2 * SUB + HEADS + k + 1]
                    enter = jnp.where(row == k, a_k * carried + b_k, enter)
            gated[here, :] = (parts[here, :].astype(f32) + parts[there, :].astype(f32) * enter).astype(bf16)
    copies = []
    narrow = block.shape[2]
    for q in range(cols):
        w = pl.ds((q + 1) * width, width)
        for i in range(width // narrow):
            part, k = pl.ds(i * narrow, narrow), q * (width // narrow) + i
            block[k] = (dot(gated_mine[...], packed[w, part]) + dot(gated_theirs[...], received[w, part])).astype(bf16)
            copies.append(pltpu.make_async_copy(block.at[k], out.at[:, pl.ds(k * narrow, narrow)], sent.at[k]))
            copies[k].start()
    for copy in copies:
        copy.wait()


VMEM = pl.BlockSpec(memory_space=pltpu.VMEM)


HBM = pl.BlockSpec(memory_space=pltpu.HBM)
PARTS = 3
SMALL = 32
HEADS = 3
LATER = 8


def call(kernel, inputs, out_shape, scratch=(), out_specs=None, aliases=None):
    run = pl.pallas_call(
        kernel,
        out_shape=out_shape,
        out_specs=out_specs or jax.tree.map(lambda _: VMEM, out_shape),
        scratch_shapes=list(scratch),
        compiler_params=pltpu.CompilerParams(vmem_limit_bytes=32 * 1024 * 1024),
        in_specs=[VMEM] * inputs[0] + [HBM] * inputs[1],
        input_output_aliases=aliases or {},
    )

    def place(i, a):
        return pltpu.with_memory_space_constraint(a, pltpu.VMEM if i < inputs[0] else pltpu.HBM)

    return lambda *args: run(*(place(i, a) for i, a in enumerate(args)))


def step(
    tokens,
    norm_gain,
    in_weight,
    gate_weight,
    conv_weight,
    decay_gate_weight,
    decay_gate_bias,
    input_gate_weight,
    input_gate_bias,
    channel_decay_rate,
    forgetting_offset,
    out_weight,
):
    half, features = tokens.shape
    length = 2 * half
    width = in_weight.shape[1]
    heads, block = decay_gate_weight.shape[:2]
    count = lax.axis_size(SP)
    plane = lax.axis_size(PLANE)
    deep = lax.axis_size("sp_0")
    S = jax.ShapeDtypeStruct

    swap = [(0, 1), (1, 0)]
    other = lax.ppermute(tokens, "tp", swap)

    row = lambda v: v.reshape(1, -1)
    later = (
        gate_weight, conv_weight, decay_gate_weight, row(decay_gate_bias),
        input_gate_weight, row(input_gate_bias), row(channel_decay_rate), forgetting_offset,
    )
    big = pltpu.VMEM
    like = lambda a: big(a.shape, a.dtype)
    square = big((length, width), f32)
    stats = [big((half, 128), f32), big((half, 128), f32)]
    gain = row(norm_gain)
    inner_own, normed_own, gain, w_in = call(
        own_tokens_kernel,
        (0, 3),
        (big((half, width), bf16), big((half, features), bf16), like(gain), like(in_weight)),
        scratch=[like(tokens), pltpu.SemaphoreType.DMA((4,)), *stats],
    )(gain, in_weight, tokens)
    inner, tail, normed_other, *held = call(
        other_tokens_kernel,
        (4, LATER),
        (
            big((length, width), bf16), big((HALO, width), bf16), big((half, features), bf16),
            *(like(a) for a in later),
        ),
        scratch=[pltpu.SemaphoreType.DMA((LATER,)), *stats],
    )(other, gain, w_in, inner_own, *later)
    w_gate, conv, w_decay, b_decay, w_input, b_input, rate, offset = held
    halo = lax.ppermute(tail, SP, [(s, s + 1) for s in range(count - 1)])
    taps = conv_weight.shape[0]
    cols = features // width
    packed_shape = big(((cols + 1) * width + PARTS * SMALL, width), bf16)
    half_square = big((length, width), bf16)
    mine, packed, ends, blocks, shift = call(
        scan_kernel,
        (11, 1),
        (
            half_square, packed_shape, big((2, SUB, width), f32),
            big((heads * block // 256, 256, 512), bf16), big((HALO * SUB, width), f32),
        ),
        scratch=[
            half_square, square, square, square,
            big((length + (taps - 1) * SUB, width), f32), half_square,
            square, square, half_square, half_square, pltpu.SemaphoreType.DMA((cols,)),
        ],
    )(
        inner, normed_own, normed_other, w_gate, conv, w_decay, b_decay, w_input, b_input, rate, offset, out_weight,
    )
    small, packed, sent = call(
        pack_kernel,
        (10, 0),
        (big((SMALL, width), f32), packed_shape, big((plane, 2, width), f32)),
        scratch=[
            big((2 * HALO, width), f32), big((2 * HALO, width), bf16),
            big((HALO, width), f32), big((HALO, width), f32),
        ],
        aliases={9: 1},
    )(inner, halo, conv, blocks, b_decay, b_input, rate, shift, ends, packed)
    received = lax.ppermute(packed, "tp", swap)
    pieces = lax.all_to_all(sent, PLANE, split_axis=0, concat_axis=0, tiled=True)
    before, sent = call(plane_kernel, (1, 0), (big((2, width), f32), big((2 * deep, 2, width), f32)))(pieces)
    pieces = lax.all_to_all(sent, ("sp_0", "tp"), split_axis=0, concat_axis=0, tiled=True)
    return call(
        out_kernel,
        (6, 0),
        S((half, features), bf16),
        scratch=(
            big((deep, 2, width), f32), big((cols, half, width), bf16),
            big((half, width), bf16), big((half, width), bf16), pltpu.SemaphoreType.DMA((cols,)),
        ),
        out_specs=HBM,
    )(pieces, before, small, mine, packed, received)


def solution(mesh):
    torus = Mesh(mesh.devices.reshape(8, 8, 4, mesh.shape["tp"]), SP_TP)
    placed = (
        P(SP_TP, None),
        P(),
        P(None, "tp"),
        P(None, "tp"),
        P(None, "tp"),
        P("tp", None, None),
        P("tp"),
        P("tp", None, None),
        P("tp"),
        P("tp"),
        P("tp", SP),
        P("tp", None),
    )
    return jax.shard_map(step, mesh=torus, in_specs=placed, out_specs=P(SP_TP, None), check_vma=False)
```
